32 devices in a mesh: sp: 8 (over z, y), tp: 4 (over x, core).
Axes of the slice: x: 2, y: 2, z: 4, core: 2. Of those that a mesh axis runs over, the one named last changes fastest.
Arguments:
- tokens: bfloat16 [4096, 2048], P('sp', 'tp'), may hold values from -6 to 6
- norm_gain: float32 [2048], replicated, may hold values from 0.1 to 1.9
- query_weight: bfloat16 [2048, 2048], P('sp', 'tp'), may hold values from -0.125 to 0.125
- key_weight: bfloat16 [2048, 512], P('sp', 'tp'), may hold values from -0.125 to 0.125
- value_weight: bfloat16 [2048, 512], P('sp', 'tp'), may hold values from -0.125 to 0.125
- pool_in_weight: bfloat16 [2048, 1024], P('sp', 'tp'), may hold values from -0.125 to 0.125
- pool_mix_weight: bfloat16 [4, 256, 256], P('tp'), may hold values from -0.375 to 0.375
- sink_logit: float32 [32], P('tp'), may hold values from -300 to 300
- out_pool_weight: bfloat16 [1024, 2048], P('tp', 'sp'), may hold values from -0.109375 to 0.109375
- out_attn_weight: bfloat16 [2048, 2048], P('tp', 'sp'), may hold values from -1.25 to 1.25
Outputs:
- mixed: bfloat16 [4096, 2048], P('sp', 'tp')
- log_weight: float32 [32, 4096], P('tp', 'sp')
The draws below stay inside these ranges and needn't reach their ends.
All inputs are finite; a program needn't handle non-finite values.
Results may differ from the reference program's by a relative error of at most 0.012.
Values may be sent and summed in bfloat16 or wider, within the bound.
No kernel may reach another device: no remote copies, remote signals or barrier semaphores. Data moves between devices by JAX's collectives and lax.ppermute only.
A program may use at most 64 MiB of HBM per device.

```python
import jax
import jax.numpy as jnp
from jax import lax

D = 2048
HQ = 32
KVH = 8
HD = 64
GROUPS = 4
POOL_GC = 256
WINDOW = 128
GRID_W = 64
POOL_WIDTH = 1024
TOKENS = 4096
N_TP = 4


def draw_sink_logit(key, part):
    heads_per_group = HQ // KVH
    drawn = jax.random.uniform(jax.random.fold_in(key, 11), (KVH, heads_per_group), jnp.float32, 2.0, 6.0)
    return drawn.reshape(HQ)


def block_scale(key, shape, cuts, low, largest):
    gain, own = 1.0, jax.random.fold_in(key, 6)
    for position, parts in cuts:
        heights = jnp.exp(jax.random.uniform(jax.random.fold_in(own, position), (parts,), jnp.float32, low / len(cuts), largest / len(cuts)))
        gain = gain * jnp.repeat(heights, shape[position] // parts).reshape([-1 if axis == position else 1 for axis in range(len(shape))])
    return gain


def scatter_about(stream_key, dims, spread, bound, pieces=(), kind=jnp.bfloat16):
    values = jax.random.normal(stream_key, dims, jnp.float32) * spread
    if len(pieces) > 0:
        values = block_scale(stream_key, dims, pieces, -0.22, 0.18) * values
    return jnp.clip(values, min=-bound, max=bound).astype(kind)


def setup_inputs(seed: int = 0) -> dict:
    streams_of = jax.random.split(jax.random.key(seed), 11)
    tokens = scatter_about(streams_of[0], (TOKENS, D), 1.0, 6.0, ((0, 8), (1, 4)))
    norm_gain = jnp.clip(1.0 + 0.18 * jax.random.normal(streams_of[1], (D,), jnp.float32), 0.1, 1.9)
    query_weight = scatter_about(streams_of[2], (D, HQ * HD), D ** -0.5, 0.125, ((0, 8), (1, 4)))
    key_weight = scatter_about(streams_of[3], (D, KVH * HD), D ** -0.5, 0.125, ((0, 8), (1, 4)))
    value_weight = scatter_about(streams_of[4], (D, KVH * HD), D ** -0.5, 0.125, ((0, 8), (1, 4)))
    pool_in_weight = scatter_about(streams_of[5], (D, POOL_WIDTH), D ** -0.5, 0.125, ((0, 8), (1, 4)))
    pool_mix_weight = scatter_about(streams_of[6], (GROUPS, POOL_GC, POOL_GC), POOL_GC ** -0.5, 0.375, ((0, 4),))
    sink_logit = draw_sink_logit(jax.random.fold_in(streams_of[10], 71), 0)
    out_pool_weight = scatter_about(streams_of[8], (POOL_WIDTH, D), (POOL_WIDTH + HQ * HD) ** -0.5, 0.109375, ((0, 4), (1, 8)))
    out_attn_weight = scatter_about(streams_of[9], (HQ * HD, D), ((POOL_WIDTH + HQ * HD) // 144) ** -0.5, 1.25, ((0, 4), (1, 8)))
    return {"tokens": tokens, "norm_gain": norm_gain, "query_weight": query_weight, "key_weight": key_weight, "value_weight": value_weight, "pool_in_weight": pool_in_weight, "pool_mix_weight": pool_mix_weight, "sink_logit": sink_logit, "out_pool_weight": out_pool_weight, "out_attn_weight": out_attn_weight}


norm_eps = 1e-06
rope_base = 10000.0
pool_reach = 8
neg_fill = -1e+30

def rope_tables(positions, head_dim):
    n_freq = head_dim // 4
    freqs = rope_base ** (-jnp.arange(n_freq, dtype=jnp.float32) / n_freq)
    rows = (positions // GRID_W).astype(jnp.float32)
    columns = (positions % GRID_W).astype(jnp.float32)
    row_angle = rows[:, None] * freqs[None, :]
    col_angle = columns[:, None] * freqs[None, :]
    return (jnp.cos(row_angle), jnp.sin(row_angle), jnp.cos(col_angle), jnp.sin(col_angle))

def rotate_half(values, cosine, sine):
    middle = values.shape[-1] // 2
    first = values[..., :middle]
    second = values[..., middle:]
    return jnp.concatenate([first * cosine - second * sine, second * cosine + first * sine], -1)

def rotate_heads(values, tables, head_dim):
    rows_count = values.shape[0]
    shaped = values.astype(jnp.float32).reshape(rows_count, -1, head_dim)
    cos_r, sin_r, cos_c, sin_c = [table[:, None, :] for table in tables]
    split = head_dim // 2
    turned = jnp.concatenate([rotate_half(shaped[..., :split], cos_r, sin_r), rotate_half(shaped[..., split:], cos_c, sin_c)], -1)
    return turned.reshape(rows_count, -1).astype(jnp.bfloat16)

def pool_group(extended, own, positions, half_width, seq_total):
    rows_count = own.shape[0]
    summed = jnp.zeros(own.shape, jnp.float32)
    counted = jnp.zeros((rows_count,), jnp.float32)
    for shift_by in range(-pool_reach, pool_reach):
        source = positions + shift_by
        inside = (shift_by >= -half_width) & (shift_by < half_width) & (source >= 0) & (source < seq_total)
        window_rows = extended[pool_reach + shift_by:pool_reach + shift_by + rows_count].astype(jnp.float32)
        summed = summed + jnp.where(inside[:, None], window_rows, 0.0)
        counted = counted + inside.astype(jnp.float32)
    return (summed / counted[:, None] - own.astype(jnp.float32)).astype(jnp.bfloat16)

def attend_block(queries, keys, values, sink, query_pos, key_pos, seq_total):
    scores = jnp.einsum('qhgd,khd->hgqk', queries.astype(jnp.float32), keys.astype(jnp.float32)) * HD ** (-0.5)
    valid = (jnp.abs(query_pos[:, None] - key_pos[None, :]) <= WINDOW) & (key_pos >= 0)[None, :] & (key_pos < seq_total)[None, :]
    scores = jnp.where(valid, scores, neg_fill)
    row_top = jnp.maximum(lax.optimization_barrier(jnp.max(scores, -1)), sink[:, :, None])
    exps = jnp.exp(scores - row_top[..., None])
    row_total = lax.optimization_barrier(jnp.sum(exps, -1)) + jnp.exp(sink[:, :, None] - row_top)
    weights = (exps / row_total[..., None]).astype(jnp.bfloat16)
    attended = jnp.einsum('hgqk,khd->qhgd', weights.astype(jnp.float32), values.astype(jnp.float32))
    return (attended.astype(jnp.bfloat16), row_top + jnp.log(row_total))

def reference(tokens, norm_gain, query_weight, key_weight, value_weight, pool_in_weight, pool_mix_weight, sink_logit, out_pool_weight, out_attn_weight):
    seq_total = tokens.shape[0]
    wide = tokens.astype(jnp.float32)
    normed = (wide * lax.rsqrt(lax.optimization_barrier(jnp.mean(wide * wide, -1, keepdims=True)) + norm_eps) * norm_gain).astype(jnp.bfloat16)
    query = jnp.dot(normed, query_weight, preferred_element_type=jnp.float32).astype(jnp.bfloat16)
    key = jnp.dot(normed, key_weight, preferred_element_type=jnp.float32).astype(jnp.bfloat16)
    value = jnp.dot(normed, value_weight, preferred_element_type=jnp.float32).astype(jnp.bfloat16)
    pool_input = jnp.dot(normed, pool_in_weight, preferred_element_type=jnp.float32).astype(jnp.bfloat16)
    positions = jnp.arange(seq_total, dtype=jnp.int32)
    tables = rope_tables(positions, HD)
    rot_query = rotate_heads(query, tables, HD)
    rot_key = rotate_heads(key, tables, HD)
    pool_parts = []
    for group in range(GROUPS):
        own = pool_input[:, group * POOL_GC:(group + 1) * POOL_GC]
        extended = jnp.pad(own, ((pool_reach, pool_reach), (0, 0)))
        pooled = pool_group(extended, own, positions, 2 ** group, seq_total)
        pool_parts.append(jnp.dot(pooled, pool_mix_weight[group], preferred_element_type=jnp.float32).astype(jnp.bfloat16))
    pool_out = jnp.concatenate(pool_parts, 1)
    grp = HQ // KVH
    query_heads = rot_query.reshape(seq_total, KVH, grp, HD)
    key_pad = jnp.pad(rot_key.reshape(seq_total, KVH, HD), ((WINDOW, WINDOW), (0, 0), (0, 0)))
    value_pad = jnp.pad(value.reshape(seq_total, KVH, HD), ((WINDOW, WINDOW), (0, 0), (0, 0)))
    sink = sink_logit.reshape(KVH, grp)
    block_rows = 512

    def block_fn(block_index):
        start = (block_index * block_rows).astype(jnp.int32)
        queries = lax.dynamic_slice_in_dim(query_heads, start, block_rows, 0)
        keys = lax.dynamic_slice_in_dim(key_pad, start, block_rows + 2 * WINDOW, 0)
        values = lax.dynamic_slice_in_dim(value_pad, start, block_rows + 2 * WINDOW, 0)
        query_pos = start + jnp.arange(block_rows, dtype=jnp.int32)
        key_pos = start - WINDOW + jnp.arange(block_rows + 2 * WINDOW, dtype=jnp.int32)
        return attend_block(queries, keys, values, sink, query_pos, key_pos, seq_total)
    n_blocks = seq_total // block_rows
    attended, log_blocks = lax.map(block_fn, jnp.arange(n_blocks, dtype=jnp.int32))
    attended = attended.reshape(seq_total, HQ * HD)
    log_weight = jnp.moveaxis(log_blocks.reshape(n_blocks, HQ, block_rows), 0, 1).reshape(HQ, seq_total)
    attn_group = HQ * HD // N_TP
    mixed = jnp.zeros((seq_total, D), jnp.float32)
    for part in range(N_TP):
        term = jnp.dot(pool_out[:, part * POOL_GC:(part + 1) * POOL_GC], out_pool_weight[part * POOL_GC:(part + 1) * POOL_GC], preferred_element_type=jnp.float32)
        term = term + jnp.dot(attended[:, part * attn_group:(part + 1) * attn_group], out_attn_weight[part * attn_group:(part + 1) * attn_group], preferred_element_type=jnp.float32)
        rounded = lax.optimization_barrier(term.astype(jnp.bfloat16))
        mixed = mixed + rounded.astype(jnp.float32)
    return (mixed.astype(jnp.bfloat16), log_weight)
```

```python
import functools

import jax
import jax.numpy as jnp
from jax import lax
from jax.experimental import pallas as pl
from jax.experimental.pallas import tpu as pltpu
from jax.sharding import PartitionSpec as P

HD = 64
WINDOW = 128
GRID_W = 64


norm_eps = 1e-06
rope_base = 10000.0
pool_reach = 8
neg_fill = -1e30


def with_halo(cells, sides, width):
    for axis, dim in sides:
        count = lax.axis_size(axis)
        ends = count - 1
        head = lax.slice_in_dim(cells, 0, width, axis=dim)
        tail = lax.slice_in_dim(cells, cells.shape[dim] - width, cells.shape[dim], axis=dim)
        cells = jnp.concatenate(
            [
                lax.ppermute(tail, axis, [(i, (i + 1) % count) for i in range(ends)]),
                cells,
                lax.ppermute(head, axis, [((i + 1) % count, i) for i in range(ends)]),
            ],
            axis=dim,
        )
    return cells


def rope_tables(positions, head_dim):
    n_freq = head_dim // 4
    freqs = rope_base ** (-jnp.arange(n_freq, dtype=jnp.float32) / n_freq)
    rows = (positions // GRID_W).astype(jnp.float32)
    columns = (positions % GRID_W).astype(jnp.float32)
    row_angle = rows[:, None] * freqs[None, :]
    col_angle = columns[:, None] * freqs[None, :]
    return (jnp.cos(row_angle), jnp.sin(row_angle), jnp.cos(col_angle), jnp.sin(col_angle))


def rotate_half(values, cosine, sine):
    middle = values.shape[-1] // 2
    first = values[..., :middle]
    second = values[..., middle:]
    return jnp.concatenate([first * cosine - second * sine, second * cosine + first * sine], -1)


def rotate_heads(values, tables, head_dim):
    rows_count = values.shape[0]
    shaped = values.astype(jnp.float32).reshape(rows_count, -1, head_dim)
    cos_r, sin_r, cos_c, sin_c = [table[:, None, :] for table in tables]
    split = head_dim // 2
    turned = jnp.concatenate(
        [
            rotate_half(shaped[..., :split], cos_r, sin_r),
            rotate_half(shaped[..., split:], cos_c, sin_c),
        ],
        -1,
    )
    return turned.reshape(rows_count, -1).astype(jnp.bfloat16)


def pool_group(extended, own, positions, half_width, seq_total):
    rows_count = own.shape[0]
    summed = jnp.zeros(own.shape, jnp.float32)
    counted = jnp.zeros((rows_count,), jnp.float32)
    for shift_by in range(-pool_reach, pool_reach):
        source = positions + shift_by
        inside = (
            (shift_by >= -half_width)
            & (shift_by < half_width)
            & (source >= 0)
            & (source < seq_total)
        )
        window_rows = extended[pool_reach + shift_by : pool_reach + shift_by + rows_count].astype(
            jnp.float32
        )
        summed = summed + jnp.where(inside[:, None], window_rows, 0.0)
        counted = counted + inside.astype(jnp.float32)
    return (summed / counted[:, None] - own.astype(jnp.float32)).astype(jnp.bfloat16)


def attend_block(queries, keys, values, sink, query_pos, key_pos, seq_total):
    scores = jnp.einsum(
        "qhgd,khd->hgqk", queries, keys, preferred_element_type=jnp.float32
    ) * HD ** (-0.5)
    valid = (
        (jnp.abs(query_pos[:, None] - key_pos[None, :]) <= WINDOW)
        & (key_pos >= 0)[None, :]
        & (key_pos < seq_total)[None, :]
    )
    scores = jnp.where(valid, scores, neg_fill)
    row_top = jnp.maximum(jnp.max(scores, -1), sink[:, :, None])
    exps = jnp.exp(scores - row_top[..., None])
    row_total = jnp.sum(exps, -1) + jnp.exp(sink[:, :, None] - row_top)
    weights = (exps / row_total[..., None]).astype(jnp.bfloat16)
    attended = jnp.einsum("hgqk,khd->qhgd", weights, values, preferred_element_type=jnp.float32)
    return (attended.astype(jnp.bfloat16), row_top + jnp.log(row_total))


def attend_all(rot_query, key_ext, value_ext, sink_logit, offset, seq_total):
    tok_rows = rot_query.shape[0]
    heads_local = rot_query.shape[1] // HD
    kv_local = key_ext.shape[1] // HD
    grp = heads_local // kv_local
    query_heads = rot_query.reshape(tok_rows, kv_local, grp, HD)
    key_heads = key_ext.reshape(-1, kv_local, HD)
    value_heads = value_ext.reshape(-1, kv_local, HD)
    sink = sink_logit.reshape(kv_local, grp)
    block_rows = min(tok_rows, 256)
    attended_parts = []
    log_parts = []
    for block_index in range(tok_rows // block_rows):
        start = block_index * block_rows
        query_pos = offset + start + jnp.arange(block_rows, dtype=jnp.int32)
        key_pos = offset + start - WINDOW + jnp.arange(block_rows + 2 * WINDOW, dtype=jnp.int32)
        attended_block, log_block = attend_block(
            query_heads[start : start + block_rows],
            key_heads[start : start + block_rows + 2 * WINDOW],
            value_heads[start : start + block_rows + 2 * WINDOW],
            sink,
            query_pos,
            key_pos,
            seq_total,
        )
        attended_parts.append(attended_block.reshape(block_rows, heads_local * HD))
        log_parts.append(log_block.reshape(heads_local, block_rows))
    attended = jnp.concatenate(attended_parts, 0)
    log_weight = jnp.concatenate(log_parts, 1)
    return (attended, log_weight)


def fetch_outputs(out_pool_weight, out_attn_weight):
    return (
        lax.all_gather(out_pool_weight, "sp", axis=1, tiled=True),
        lax.all_gather(out_attn_weight, "sp", axis=1, tiled=True),
    )


def local(
    tokens,
    norm_gain,
    query_weight,
    key_weight,
    value_weight,
    pool_in_weight,
    pool_mix_weight,
    sink_logit,
    out_pool_weight,
    out_attn_weight,
):
    whole = lax.all_gather(tokens, "tp", axis=1, tiled=True)
    wide = whole.astype(jnp.float32)
    normed = (
        wide * lax.rsqrt(jnp.mean(wide * wide, -1, keepdims=True) + norm_eps) * norm_gain
    ).astype(jnp.bfloat16)
    tok_rows = normed.shape[0]
    seq_total = tok_rows * lax.axis_size("sp")
    offset = lax.axis_index("sp") * tok_rows
    weights_in = (query_weight, key_weight, value_weight, pool_in_weight)
    pieces = (
        lax.all_gather(weights_in[0], "sp", axis=0, tiled=True),
        lax.all_gather(weights_in[1], "sp", axis=0, tiled=True),
        lax.all_gather(weights_in[2], "sp", axis=0, tiled=True),
        lax.all_gather(weights_in[3], "sp", axis=0, tiled=True),
    )
    sums = tuple((jnp.dot(normed, piece, preferred_element_type=jnp.float32) for piece in pieces))
    query, key, value, pool_input = [total.astype(jnp.bfloat16) for total in sums]
    positions = offset + jnp.arange(tok_rows, dtype=jnp.int32)
    tables = rope_tables(positions, HD)
    rot_query = rotate_heads(query, tables, HD)
    rot_key = rotate_heads(key, tables, HD)
    key_width = rot_key.shape[1]
    pool_ext = with_halo(pool_input, (("sp", 0),), pool_reach)
    pair_ext = with_halo(jnp.concatenate([rot_key, value], 1), (("sp", 0),), WINDOW)
    key_ext = pair_ext[:, :key_width]
    value_ext = pair_ext[:, key_width:]
    half_width = jnp.left_shift(jnp.int32(1), lax.axis_index("tp"))
    pooled = pool_group(pool_ext, pool_input, positions, half_width, seq_total)
    pool_out = jnp.dot(pooled, pool_mix_weight[0], preferred_element_type=jnp.float32).astype(
        jnp.bfloat16
    )
    attended, log_weight = attend_all(rot_query, key_ext, value_ext, sink_logit, offset, seq_total)
    out_pool_full, out_attn_full = fetch_outputs(out_pool_weight, out_attn_weight)
    term = jnp.dot(pool_out, out_pool_full, preferred_element_type=jnp.float32)
    term = term + jnp.dot(attended, out_attn_full, preferred_element_type=jnp.float32)
    mixed = lax.psum_scatter(term.astype(jnp.bfloat16), "tp", scatter_dimension=1, tiled=True)
    return (mixed, log_weight)


def make_perm(planes, rule):
    pairs = []
    for z in range(planes):
        for y in range(2):
            for x in range(2):
                for c in range(2):
                    to = rule(z, y, x, c)
                    if to is not None:
                        pairs.append((lin(z, y, x, c), lin(*to)))
    return pairs


def lin(z, y, x, c):
    return ((z * 2 + y) * 2 + x) * 2 + c


def send(value, rule, planes=4):
    return lax.ppermute(value, ("sp", "tp"), make_perm(planes, rule))


def after(value, *tokens):
    return lax.optimization_barrier((value, *tokens))[0]


def swap_away(z, y, x, c):
    return (z, c, x, y) if y != c else None


def home_to_away(z, y, x, c):
    return (z, y, x, 1 - c) if y == c else None


def away_to_home(z, y, x, c):
    return (z, y, x, 1 - c) if y != c else None


def other_core(z, y, x, c):
    return (z, y, x, 1 - c)


def line_one(z, y, x, c):
    if c == 0:
        return (z + 1, y, x, c) if z < 3 else None
    return (z - 1, y, x, c) if z > 0 else None


def line_two(core):
    def rule(z, y, x, c):
        if z not in (1, 2):
            return None
        return (z + 1 if c == 0 else z - 1, y, x, core)

    return rule


def line_three(core):
    def rule(z, y, x, c):
        if c != core or z not in (1, 2):
            return None
        return (0 if z == 1 else 3, y, x, c)

    return rule


def token_one(z, y, x, c):
    return (z, y, 1 - x, c) if y == c else (z, 1 - y, x, 1 - c)


def token_two(z, y, x, c):
    return (z, y, 1 - x, 1 - c) if y != c else (z, 1 - y, x, c)


def token_diag(z, y, x, c):
    return (z, y, 1 - x, c) if y != c else None


def halo_next(z, y, x, c):
    if c == 0:
        return (z, y, x, 1)
    return (z + 1, y, x, 0) if z < 3 else None


def halo_prev(z, y, x, c):
    if c == 1:
        return (z, y, x, 0)
    return (z - 1, y, x, 1) if z > 0 else None


def norm_kernel(idx, own, p1, p2, p3, p4, p5, gain, out, buf, sems):
    home = idx[0]
    places = [idx[1], idx[2], idx[3], idx[4]]
    at_home = (own, p3, p1, p2)
    at_away = (p2, p1, p5, p4)
    for which in range(4):

        @pl.when(home == 1)
        def _():
            pltpu.make_async_copy(at_home[which], buf.at[places[which]], sems.at[which]).start()

        @pl.when(home == 0)
        def _():
            pltpu.make_async_copy(at_away[which], buf.at[places[which]], sems.at[which]).start()

    for which in range(4):
        pltpu.make_async_copy(own, buf.at[places[which]], sems.at[which]).wait()
    blocks, rows, wide = buf.shape
    half = wide // 2
    step = 128

    def body(i, carry):
        at = pl.ds(pl.multiple_of(i * step, step), step)
        total = jnp.zeros((step, 1), jnp.float32)
        for b in range(blocks):
            v = buf[b, at, :].astype(jnp.float32)
            total = total + jnp.sum(v * v, -1, keepdims=True)
        scale = lax.rsqrt(total / (blocks * wide) + norm_eps)
        for b in range(blocks):
            v = buf[b, at, :].astype(jnp.float32)
            buf[b, at, :] = (v * scale * gain[:, b * wide : (b + 1) * wide]).astype(jnp.bfloat16)
        for slot in range(out.shape[0]):
            fb = idx[5 + slot]
            col = pl.multiple_of((fb % 2) * half, half)
            out[slot, at, :] = buf[fb // 2, at, pl.ds(col, half)]
        return carry

    lax.fori_loop(0, rows // step, body, 0)


def normed_slots(idx, pieces, gain, slots):
    rows, wide = pieces[0].shape
    anyspace = pl.BlockSpec(memory_space=pl.ANY)
    return pl.pallas_call(
        norm_kernel,
        out_shape=jax.ShapeDtypeStruct((slots, rows, wide // 2), jnp.bfloat16),
        in_specs=[pl.BlockSpec(memory_space=pltpu.SMEM)] + [anyspace] * 6 + [pl.BlockSpec(memory_space=pltpu.VMEM)],
        out_specs=pl.BlockSpec(memory_space=pltpu.VMEM),
        scratch_shapes=[pltpu.VMEM((4, rows, wide), jnp.bfloat16), pltpu.SemaphoreType.DMA((4,))],
        name="norm",
    )(idx, *pieces, gain)


def gather_dot(first, has_acc, *refs):
    normed = refs[0]
    count = len(refs) - 2 - (1 if has_acc else 0)
    weights = refs[1 : 1 + count]
    out = refs[-1]
    rows = normed.shape[1]
    step = 256
    for at in range(0, rows, step):
        total = refs[1 + count][at : at + step] if has_acc else None
        for i in range(count):
            part = jnp.dot(normed[first + i, at : at + step, :], weights[i][...], preferred_element_type=jnp.float32)
            total = part if total is None else total + part
        out[at : at + step] = total


def project(normed, first, weights, acc):
    rows = normed.shape[1]
    cols = weights[0].shape[1]
    args = (normed, *weights) + (() if acc is None else (acc,))
    return pl.pallas_call(
        functools.partial(gather_dot, first, acc is not None),
        out_shape=jax.ShapeDtypeStruct((rows, cols), jnp.float32),
        name="project",
    )(*args)


def out_kernel(first, count, idx, acts, *refs):
    weights = refs[:count]
    outs = refs[-4:]
    for i in range(count):
        place = idx[first + i]
        result = jnp.dot(acts[...], weights[i][...], preferred_element_type=jnp.float32).astype(jnp.bfloat16)
        half = result.shape[1]
        col = pl.multiple_of((place % 2) * half, half)
        for r in range(4):

            @pl.when(place // 2 == r)
            def _():
                outs[r][:, pl.ds(col, half)] = result


def out_blocks(idx, acts, weights):
    rows = acts.shape[0]
    wide = weights[0].shape[1] * 2
    count = len(weights)
    return pl.pallas_call(
        functools.partial(out_kernel, 0, count),
        out_shape=[jax.ShapeDtypeStruct((rows, wide), jnp.bfloat16)] * 4,
        in_specs=[pl.BlockSpec(memory_space=pltpu.SMEM)] + [pl.BlockSpec(memory_space=pltpu.VMEM)] * (1 + count),
        out_specs=[pl.BlockSpec(memory_space=pltpu.VMEM)] * 4,
        name="outproj",
    )(idx, acts, *weights)


def line_gather(own, swapped, home, core):
    near = jnp.where(home, own, send(own, home_to_away))
    d1 = send(near, line_one)
    far = jnp.where(home, send(swapped, away_to_home), swapped)
    s1 = send(far, line_one)
    d2 = send(d1, line_two(0))
    s2 = send(s1, line_two(1))
    d3 = send(d2, line_three(0))
    s3 = send(s2, line_three(1))
    w2 = jnp.where(core == 0, d2, s2)
    w3 = jnp.where(core == 0, d3, s3)
    return (near, far, d1, s1, send(d1, other_core), send(s1, other_core), w2, send(w2, other_core), w3, send(w3, other_core))


def local_lines(
    tokens,
    norm_gain,
    query_weight,
    key_weight,
    value_weight,
    pool_in_weight,
    pool_mix_weight,
    sink_logit,
    out_pool_weight,
    out_attn_weight,
):
    s, t = lax.axis_index("sp"), lax.axis_index("tp")
    z, y, x, c = s // 2, s % 2, t // 2, t % 2
    home = y == c
    planes = lax.axis_size("sp") // 2
    tok_rows = tokens.shape[0]
    seq_total = tok_rows * lax.axis_size("sp")
    offset = (2 * z + c) * tok_rows

    w_in = jnp.concatenate([query_weight, key_weight, value_weight, pool_in_weight], 1)
    in_swapped = send(w_in, swap_away)
    w_slots = line_gather(w_in, in_swapped, home, c)

    p1 = send(tokens, token_one)
    p2 = send(tokens, token_two)
    p3 = send(tokens, away_to_home)
    p4 = send(p1, token_diag)
    p5 = send(p2, token_diag)

    w_out = jnp.concatenate([out_pool_weight, out_attn_weight, pool_mix_weight[0]], 0)
    out_swapped = send(w_out, swap_away)
    sink_other = send(sink_logit, swap_away)
    mix_rows = pool_mix_weight.shape[1]
    cut = w_out.shape[0] - mix_rows
    mix = jnp.where(home, w_out[cut:], out_swapped[cut:])
    sink_own = jnp.where(home, sink_logit, sink_other)
    o_slots = line_gather(w_out[:cut], out_swapped[:cut], home, c)

    zr = jnp.where(c == 0, z - 1, z + 1)
    ze = jnp.where(c == 0, z + 1, z - 1)
    z2 = jnp.where(z < planes // 2, z + 2, z - 2)
    z3 = planes - 1 - z
    yc = (y + c) % 2
    feature = jnp.stack(
        [
            2 * z + y,
            2 * z + 1 - y,
            2 * zr + y,
            2 * zr + 1 - y,
            2 * ze + y,
            2 * ze + 1 - y,
            2 * z2 + yc,
            2 * z2 + 1 - yc,
            2 * z3 + yc,
            2 * z3 + 1 - yc,
        ]
    )
    outer = (z == 0) | (z == planes - 1)
    zs = jnp.stack([z, z, zr, zr, ze, ze, z2, z2, jnp.where(outer, z3, -1), jnp.where(outer, z3, -1)])
    valid = (zs >= 0) & (zs < planes)
    fb = jnp.where(valid, feature, 0).astype(jnp.int32)
    head = jnp.stack([home.astype(jnp.int32), 2 * x + c, 2 * x + 1 - c, 2 * (1 - x) + c, 2 * (1 - x) + 1 - c]).astype(jnp.int32)
    normed = normed_slots(jnp.concatenate([head, fb]), (tokens, p1, p2, p3, p4, p5), norm_gain[None, :], 10)

    acc = project(normed, 0, w_slots[:6], None)
    sums = project(normed, 6, w_slots[6:], acc).astype(jnp.bfloat16)
    q_w, kv_w = query_weight.shape[1], key_weight.shape[1]
    query = sums[:, :q_w]
    key = sums[:, q_w : q_w + kv_w]
    value = sums[:, q_w + kv_w : q_w + 2 * kv_w]
    pool_input = sums[:, q_w + 2 * kv_w :]

    positions = offset + jnp.arange(tok_rows, dtype=jnp.int32)
    tables = rope_tables(positions, HD)
    rot_query = rotate_heads(query, tables, HD)
    rot_key = rotate_heads(key, tables, HD)
    pair = jnp.concatenate([rot_key, value], 1)
    low = jnp.concatenate([pair[:WINDOW], pool_input[:pool_reach]], 0)
    high = jnp.concatenate([pair[tok_rows - WINDOW :], pool_input[tok_rows - pool_reach :]], 0)
    before = send(high, halo_next)
    behind = send(low, halo_prev)
    pair_ext = jnp.concatenate([before[:WINDOW], pair, behind[:WINDOW]], 0)
    pool_ext = jnp.concatenate([before[WINDOW:], pool_input, behind[WINDOW:]], 0)
    half_width = jnp.left_shift(jnp.int32(1), 2 * x + y)
    pooled = pool_group(pool_ext, pool_input, positions, half_width, seq_total)
    pool_out = jnp.dot(pooled, mix, preferred_element_type=jnp.float32).astype(jnp.bfloat16)
    attended, log_here = attend_all(rot_query, pair_ext[:, :kv_w], pair_ext[:, kv_w:], sink_own, offset, seq_total)
    log_weight = jnp.where(home, log_here, send(log_here, swap_away))

    acts = jnp.concatenate([pool_out, attended], 1)
    round_of = lambda zz: zz ^ (2 * x + y)
    parity = fb % 2
    place = jnp.where(valid, (zs ^ (2 * x + y)) * 2 + parity, -2).astype(jnp.int32)
    blocks = out_blocks(place, acts, o_slots)

    def direct(r):
        def rule(z, y, x, c):
            j = (2 * x + y) ^ r
            to = (z, c, j // 2, j % 2)
            return None if to == (z, y, x, c) else to

        return rule

    parts = [send(blocks[r], direct(r)) for r in range(4)]
    parts[0] = jnp.where(home, blocks[0], parts[0])
    mixed = sum(part.astype(jnp.float32) for part in parts).astype(jnp.bfloat16)
    return (mixed, log_weight)


def solution(mesh):
    lines = mesh.shape["sp"] == 8 and mesh.shape["tp"] == 4
    return jax.shard_map(
        local_lines if lines else local,
        mesh=mesh,
        in_specs=(
            P("sp", "tp"),
            P(),
            P("sp", "tp"),
            P("sp", "tp"),
            P("sp", "tp"),
            P("sp", "tp"),
            P("tp", None, None),
            P("tp"),
            P("tp", "sp"),
            P("tp", "sp"),
        ),
        out_specs=(P("sp", "tp"), P("tp", "sp")),
        check_vma=False,
    )
```

```python
import functools

import jax
import jax.numpy as jnp
from jax import lax
from jax.experimental import pallas as pl
from jax.experimental.pallas import tpu as pltpu
from jax.sharding import PartitionSpec as P

HD = 64
WINDOW = 128
GRID_W = 64


norm_eps = 1e-06
rope_base = 10000.0
pool_reach = 8
neg_fill = -1e30


def with_halo(cells, sides, width):
    for axis, dim in sides:
        count = lax.axis_size(axis)
        ends = count - 1
        head = lax.slice_in_dim(cells, 0, width, axis=dim)
        tail = lax.slice_in_dim(cells, cells.shape[dim] - width, cells.shape[dim], axis=dim)
        cells = jnp.concatenate(
            [
                lax.ppermute(tail, axis, [(i, (i + 1) % count) for i in range(ends)]),
                cells,
                lax.ppermute(head, axis, [((i + 1) % count, i) for i in range(ends)]),
            ],
            axis=dim,
        )
    return cells


def rope_tables(positions, head_dim):
    n_freq = head_dim // 4
    freqs = rope_base ** (-jnp.arange(n_freq, dtype=jnp.float32) / n_freq)
    rows = (positions // GRID_W).astype(jnp.float32)
    columns = (positions % GRID_W).astype(jnp.float32)
    row_angle = rows[:, None] * freqs[None, :]
    col_angle = columns[:, None] * freqs[None, :]
    return (jnp.cos(row_angle), jnp.sin(row_angle), jnp.cos(col_angle), jnp.sin(col_angle))


def rotate_half(values, cosine, sine):
    middle = values.shape[-1] // 2
    first = values[..., :middle]
    second = values[..., middle:]
    return jnp.concatenate([first * cosine - second * sine, second * cosine + first * sine], -1)


def rotate_heads(values, tables, head_dim):
    rows_count = values.shape[0]
    shaped = values.astype(jnp.float32).reshape(rows_count, -1, head_dim)
    cos_r, sin_r, cos_c, sin_c = [table[:, None, :] for table in tables]
    split = head_dim // 2
    turned = jnp.concatenate(
        [
            rotate_half(shaped[..., :split], cos_r, sin_r),
            rotate_half(shaped[..., split:], cos_c, sin_c),
        ],
        -1,
    )
    return turned.reshape(rows_count, -1).astype(jnp.bfloat16)


def pool_group(extended, own, positions, half_width, seq_total):
    rows_count = own.shape[0]
    summed = jnp.zeros(own.shape, jnp.float32)
    counted = jnp.zeros((rows_count,), jnp.float32)
    for shift_by in range(-pool_reach, pool_reach):
        source = positions + shift_by
        inside = (
            (shift_by >= -half_width)
            & (shift_by < half_width)
            & (source >= 0)
            & (source < seq_total)
        )
        window_rows = extended[pool_reach + shift_by : pool_reach + shift_by + rows_count].astype(
            jnp.float32
        )
        summed = summed + jnp.where(inside[:, None], window_rows, 0.0)
        counted = counted + inside.astype(jnp.float32)
    return (summed / counted[:, None] - own.astype(jnp.float32)).astype(jnp.bfloat16)


def attend_block(queries, keys, values, sink, query_pos, key_pos, seq_total):
    scores = jnp.einsum(
        "qhgd,khd->hgqk", queries, keys, preferred_element_type=jnp.float32
    ) * HD ** (-0.5)
    valid = (
        (jnp.abs(query_pos[:, None] - key_pos[None, :]) <= WINDOW)
        & (key_pos >= 0)[None, :]
        & (key_pos < seq_total)[None, :]
    )
    scores = jnp.where(valid, scores, neg_fill)
    row_top = jnp.maximum(jnp.max(scores, -1), sink[:, :, None])
    exps = jnp.exp(scores - row_top[..., None])
    row_total = jnp.sum(exps, -1) + jnp.exp(sink[:, :, None] - row_top)
    weights = (exps / row_total[..., None]).astype(jnp.bfloat16)
    attended = jnp.einsum("hgqk,khd->qhgd", weights, values, preferred_element_type=jnp.float32)
    return (attended.astype(jnp.bfloat16), row_top + jnp.log(row_total))


def attend_all(rot_query, key_ext, value_ext, sink_logit, offset, seq_total):
    tok_rows = rot_query.shape[0]
    heads_local = rot_query.shape[1] // HD
    kv_local = key_ext.shape[1] // HD
    grp = heads_local // kv_local
    query_heads = rot_query.reshape(tok_rows, kv_local, grp, HD)
    key_heads = key_ext.reshape(-1, kv_local, HD)
    value_heads = value_ext.reshape(-1, kv_local, HD)
    sink = sink_logit.reshape(kv_local, grp)
    block_rows = min(tok_rows, 256)
    attended_parts = []
    log_parts = []
    for block_index in range(tok_rows // block_rows):
        start = block_index * block_rows
        query_pos = offset + start + jnp.arange(block_rows, dtype=jnp.int32)
        key_pos = offset + start - WINDOW + jnp.arange(block_rows + 2 * WINDOW, dtype=jnp.int32)
        attended_block, log_block = attend_block(
            query_heads[start : start + block_rows],
            key_heads[start : start + block_rows + 2 * WINDOW],
            value_heads[start : start + block_rows + 2 * WINDOW],
            sink,
            query_pos,
            key_pos,
            seq_total,
        )
        attended_parts.append(attended_block.reshape(block_rows, heads_local * HD))
        log_parts.append(log_block.reshape(heads_local, block_rows))
    attended = jnp.concatenate(attended_parts, 0)
    log_weight = jnp.concatenate(log_parts, 1)
    return (attended, log_weight)


def fetch_outputs(out_pool_weight, out_attn_weight):
    return (
        lax.all_gather(out_pool_weight, "sp", axis=1, tiled=True),
        lax.all_gather(out_attn_weight, "sp", axis=1, tiled=True),
    )


def local(
    tokens,
    norm_gain,
    query_weight,
    key_weight,
    value_weight,
    pool_in_weight,
    pool_mix_weight,
    sink_logit,
    out_pool_weight,
    out_attn_weight,
):
    whole = lax.all_gather(tokens, "tp", axis=1, tiled=True)
    wide = whole.astype(jnp.float32)
    normed = (
        wide * lax.rsqrt(jnp.mean(wide * wide, -1, keepdims=True) + norm_eps) * norm_gain
    ).astype(jnp.bfloat16)
    tok_rows = normed.shape[0]
    seq_total = tok_rows * lax.axis_size("sp")
    offset = lax.axis_index("sp") * tok_rows
    weights_in = (query_weight, key_weight, value_weight, pool_in_weight)
    pieces = (
        lax.all_gather(weights_in[0], "sp", axis=0, tiled=True),
        lax.all_gather(weights_in[1], "sp", axis=0, tiled=True),
        lax.all_gather(weights_in[2], "sp", axis=0, tiled=True),
        lax.all_gather(weights_in[3], "sp", axis=0, tiled=True),
    )
    sums = tuple((jnp.dot(normed, piece, preferred_element_type=jnp.float32) for piece in pieces))
    query, key, value, pool_input = [total.astype(jnp.bfloat16) for total in sums]
    positions = offset + jnp.arange(tok_rows, dtype=jnp.int32)
    tables = rope_tables(positions, HD)
    rot_query = rotate_heads(query, tables, HD)
    rot_key = rotate_heads(key, tables, HD)
    key_width = rot_key.shape[1]
    pool_ext = with_halo(pool_input, (("sp", 0),), pool_reach)
    pair_ext = with_halo(jnp.concatenate([rot_key, value], 1), (("sp", 0),), WINDOW)
    key_ext = pair_ext[:, :key_width]
    value_ext = pair_ext[:, key_width:]
    half_width = jnp.left_shift(jnp.int32(1), lax.axis_index("tp"))
    pooled = pool_group(pool_ext, pool_input, positions, half_width, seq_total)
    pool_out = jnp.dot(pooled, pool_mix_weight[0], preferred_element_type=jnp.float32).astype(
        jnp.bfloat16
    )
    attended, log_weight = attend_all(rot_query, key_ext, value_ext, sink_logit, offset, seq_total)
    out_pool_full, out_attn_full = fetch_outputs(out_pool_weight, out_attn_weight)
    term = jnp.dot(pool_out, out_pool_full, preferred_element_type=jnp.float32)
    term = term + jnp.dot(attended, out_attn_full, preferred_element_type=jnp.float32)
    mixed = lax.psum_scatter(term.astype(jnp.bfloat16), "tp", scatter_dimension=1, tiled=True)
    return (mixed, log_weight)


ANY = pl.BlockSpec(memory_space=pl.ANY)
SMEM = pl.BlockSpec(memory_space=pltpu.SMEM)
VMEM = pl.BlockSpec(memory_space=pltpu.VMEM)


def lin(z, y, x, c):
    return ((z * 2 + y) * 2 + x) * 2 + c


def make_perm(rule):
    pairs = []
    for z in range(4):
        for y in range(2):
            for x in range(2):
                for c in range(2):
                    to = rule(z, y, x, c)
                    if to is not None and to != (z, y, x, c):
                        pairs.append((lin(z, y, x, c), lin(*to)))
    return pairs


def send(name, value, rule):
    with jax.named_scope(name):
        return lax.ppermute(value, ("sp", "tp"), make_perm(rule))


def after(value, *tokens):
    return lax.optimization_barrier((value, *tokens))[0]


def swap_away(z, y, x, c):
    return (z, c, x, y) if y != c else None


def home_to_away(z, y, x, c):
    return (z, y, x, 1 - c) if y == c else None


def away_to_home(z, y, x, c):
    return (z, y, x, 1 - c) if y != c else None


def other_core(z, y, x, c):
    return (z, y, x, 1 - c)


def from_core(core):
    return lambda z, y, x, c: (z, y, x, 1 - c) if c == core else None


def line_one(z, y, x, c):
    if c == 0:
        return (z + 1, y, x, c) if z < 3 else None
    return (z - 1, y, x, c) if z > 0 else None


def line_two(core):
    def rule(z, y, x, c):
        if z not in (1, 2):
            return None
        return (z + 1 if c == 0 else z - 1, y, x, core)

    return rule


def line_three(core):
    def rule(z, y, x, c):
        if c != core or z not in (1, 2):
            return None
        return (0 if z == 1 else 3, y, x, c)

    return rule


def end_core(core):
    return lambda z, y, x, c: (z, y, x, 1 - c) if c == core and z in (0, 3) else None


def token_one(z, y, x, c):
    return (z, y, 1 - x, c) if y == c else (z, 1 - y, x, 1 - c)


def token_two(z, y, x, c):
    return (z, y, 1 - x, 1 - c) if y != c else (z, 1 - y, x, c)


def token_diag(z, y, x, c):
    return (z, y, 1 - x, c) if y != c else None


def halo_next(z, y, x, c):
    if c == 0:
        return (z, y, x, 1)
    return (z + 1, y, x, 0) if z < 3 else None


def halo_prev(z, y, x, c):
    if c == 1:
        return (z, y, x, 0)
    return (z - 1, y, x, 1) if z > 0 else None


def late_block(z):
    return 3 if z < 2 else 0


def part_early(r):
    def rule(z, y, x, c):
        j = (2 * x + y) ^ r
        return None if j == late_block(z) else (z, c, j // 2, j % 2)

    return rule


def part_late(r):
    def rule(z, y, x, c):
        j = (2 * x + y) ^ r
        return (z, c, j // 2, j % 2) if j == late_block(z) else None

    return rule


def pack_kernel(axis, *refs):
    sources, out, sems = refs[:-2], refs[-2], refs[-1]
    copies = []
    at = 0
    for i, source in enumerate(sources):
        size = source.shape[axis]
        span = pl.ds(at, size)
        where = (span, slice(None)) if axis == 0 else (slice(None), span)
        copies.append(pltpu.make_async_copy(source, out.at[where], sems.at[i]))
        copies[-1].start()
        at += size
    for copy in copies:
        copy.wait()


def pack(name, arrays, axis):
    shape = list(arrays[0].shape)
    shape[axis] = sum(a.shape[axis] for a in arrays)
    return pl.pallas_call(
        functools.partial(pack_kernel, axis),
        out_shape=jax.ShapeDtypeStruct(tuple(shape), arrays[0].dtype),
        in_specs=[ANY] * len(arrays),
        out_specs=ANY,
        scratch_shapes=[pltpu.SemaphoreType.DMA((len(arrays),))],
        name=name,
    )(*arrays)


def fetch(slots, buf, sems):
    for i, choices in enumerate(slots):
        for when, ref in choices:
            copy = pltpu.make_async_copy(ref, buf.at[i], sems.at[i])
            if when is None:
                copy.start()
            else:
                pl.when(when)(copy.start)


def arrived(slots, buf, sems, i):
    pltpu.make_async_copy(slots[i][0][1], buf.at[i], sems.at[i]).wait()


def norm_kernel(idx, own, p1, p2, p3, p4, p5, gain, out, buf, sems):
    home = idx[0]
    at_home = (own, p3, p1, p2)
    at_away = (p2, p1, p5, p4)
    for i in range(4):
        for when, ref in ((home == 1, at_home[i]), (home == 0, at_away[i])):
            pl.when(when)(pltpu.make_async_copy(ref, buf.at[idx[1 + i]], sems.at[i]).start)
    for i in range(4):
        pltpu.make_async_copy(own, buf.at[idx[1 + i]], sems.at[i]).wait()
    blocks, rows, wide = buf.shape
    half = wide // 2
    step = 64

    def body(i, carry):
        at = pl.ds(pl.multiple_of(i * step, step), step)
        total = jnp.zeros((step, wide), jnp.float32)
        for b in range(blocks):
            v = buf[b, at, :].astype(jnp.float32)
            total = total + v * v
        scale = lax.rsqrt(jnp.sum(total, -1, keepdims=True) / (blocks * wide) + norm_eps)
        for b in range(blocks):
            v = buf[b, at, :].astype(jnp.float32)
            v = (v * scale * gain[:, b * wide : (b + 1) * wide]).astype(jnp.bfloat16)
            out[2 * b, at, :] = v[:, :half]
            out[2 * b + 1, at, :] = v[:, half:]
        return carry

    lax.fori_loop(0, rows // step, body, 0)


def norm_tokens(idx, pieces, gain):
    rows, wide = pieces[0].shape
    return pl.pallas_call(
        norm_kernel,
        out_shape=jax.ShapeDtypeStruct((8, rows, wide // 2), jnp.bfloat16),
        in_specs=[SMEM] + [ANY] * 6 + [VMEM],
        out_specs=VMEM,
        scratch_shapes=[pltpu.VMEM((4, rows, wide), jnp.bfloat16), pltpu.SemaphoreType.DMA((4,))],
        name="norm",
    )(idx, *pieces, gain)


def near_kernel(idx, normed, near, far, d1, s1, ed1, es1, out, buf, sems):
    slots = [[(None, ref)] for ref in (near, far, d1, s1, ed1, es1)]
    fetch(slots, buf, sems)
    for pair in range(3):
        arrived(slots, buf, sems, 2 * pair)
        arrived(slots, buf, sems, 2 * pair + 1)

        def add():
            rows = normed.shape[1]
            for at in range(0, rows, rows // 2):
                span = pl.ds(at, rows // 2)
                part = jnp.dot(normed[idx[2 * pair], span, :], buf[2 * pair], preferred_element_type=jnp.float32)
                part += jnp.dot(normed[idx[2 * pair + 1], span, :], buf[2 * pair + 1], preferred_element_type=jnp.float32)
                if pair == 0:
                    out[span, :] = part
                else:
                    out[span, :] += part

        if pair == 0:
            add()
        else:
            pl.when(idx[2 * pair] >= 0)(add)


def project_near(idx, normed, slots):
    rows = normed.shape[1]
    deep, cols = slots[0].shape
    return pl.pallas_call(
        near_kernel,
        out_shape=jax.ShapeDtypeStruct((rows, cols), jnp.float32),
        in_specs=[SMEM, VMEM] + [ANY] * 6,
        out_specs=VMEM,
        scratch_shapes=[pltpu.VMEM((6, deep, cols), jnp.bfloat16), pltpu.SemaphoreType.DMA((6,))],
        name="project_near",
    )(idx, normed, *slots)


def turn(v, cosine, sine):
    lane = lax.broadcasted_iota(jnp.int32, v.shape, 1)
    quarter = HD // 4
    partner = jnp.where(lane % (2 * quarter) < quarter, pltpu.roll(v, v.shape[1] - quarter, 1), pltpu.roll(v, quarter, 1))
    return v * cosine + partner * sine


def far_kernel(widths, idx, normed, acc, cosine, sine, *refs):
    d2, s2, ed2, es2, d3, s3, ed3, es3, query, pair, pool, low, high, buf, sems = refs
    core = idx[0]
    slots = [[(core == 0, a), (core == 1, b)] for a, b in ((d2, ed2), (es2, s2), (d3, ed3), (es3, s3))]
    fetch(slots, buf, sems)
    for i in range(4):
        arrived(slots, buf, sems, i)
    rows = normed.shape[1]
    q_w, kv_w = widths
    half = rows // 2
    for at in range(0, rows, half):
        span = pl.ds(at, half)
        total = acc[span, :]
        for i in range(4):
            total += jnp.dot(normed[idx[1 + i], span, :], buf[i], preferred_element_type=jnp.float32)
        total = total.astype(jnp.bfloat16)
        co, si = cosine[span, :], sine[span, :]
        lanes = co.shape[1]
        for col in range(0, q_w + kv_w, lanes):
            v = turn(total[:, col : col + lanes].astype(jnp.float32), co, si).astype(jnp.bfloat16)
            if col < q_w:
                query[span, col : col + lanes] = v
            else:
                pair[span, col - q_w : col - q_w + lanes] = v
        pair[span, kv_w:] = total[:, q_w + kv_w : q_w + 2 * kv_w]
        pool[span, :] = total[:, q_w + 2 * kv_w :]
    low[:WINDOW, :] = pair[:WINDOW, :]
    low[WINDOW:, :] = pool[:pool_reach, :]
    high[:WINDOW, :] = pair[rows - WINDOW :, :]
    high[WINDOW:, :] = pool[rows - pool_reach :, :]


def project_far(idx, normed, acc, tables, slots, widths):
    rows = normed.shape[1]
    deep, cols = slots[0].shape
    q_w, kv_w = widths
    pool_w = cols - q_w - 2 * kv_w
    edge = (WINDOW + pool_reach, pool_w)
    return pl.pallas_call(
        functools.partial(far_kernel, widths),
        out_shape=[
            jax.ShapeDtypeStruct(shape, jnp.bfloat16)
            for shape in ((rows, q_w), (rows, 2 * kv_w), (rows, pool_w), edge, edge)
        ],
        in_specs=[SMEM] + [VMEM] * 4 + [ANY] * 8,
        out_specs=[VMEM] * 5,
        scratch_shapes=[pltpu.VMEM((4, deep, cols), jnp.bfloat16), pltpu.SemaphoreType.DMA((4,))],
        name="project_far",
    )(idx, normed, acc, *tables, *slots)


def pool_kernel(seq_total, idx, own, before, behind, mix, out, ext):
    rows, wide = own.shape
    ext[:pool_reach, :] = before[WINDOW:, :].astype(jnp.float32)
    ext[pool_reach : pool_reach + rows, :] = own[...].astype(jnp.float32)
    ext[pool_reach + rows :, :] = behind[WINDOW:, :].astype(jnp.float32)
    group, offset = idx[0], idx[1]
    position = offset + lax.broadcasted_iota(jnp.int32, (rows, 1), 0)
    for g in range(4):

        @pl.when(group == g)
        def _():
            reach = 1 << g
            total = ext[pool_reach - reach : pool_reach - reach + rows, :]
            for shift in range(1 - reach, reach):
                total = total + ext[pool_reach + shift : pool_reach + shift + rows, :]
            count = jnp.minimum(position + reach, seq_total) - jnp.maximum(position - reach, 0)
            mean = total / count.astype(jnp.float32)
            pooled = (mean - ext[pool_reach : pool_reach + rows, :]).astype(jnp.bfloat16)
            out[...] = jnp.dot(pooled, mix[...], preferred_element_type=jnp.float32).astype(jnp.bfloat16)


def pool_mixer(idx, own, before, behind, mix, seq_total):
    rows, wide = own.shape
    return pl.pallas_call(
        functools.partial(pool_kernel, seq_total),
        out_shape=jax.ShapeDtypeStruct((rows, mix.shape[1]), jnp.bfloat16),
        in_specs=[SMEM] + [VMEM] * 4,
        out_specs=VMEM,
        scratch_shapes=[pltpu.VMEM((rows + 2 * pool_reach, wide), jnp.float32)],
        name="pool",
    )(idx, own, before, behind, mix)


def attend_kernel(seq_total, idx, query, pair, before, behind, sink, out, logs, keys, values):
    rows = query.shape[0]
    lanes = 2 * HD
    block = WINDOW
    span = 3 * block
    kv_w = pair.shape[1] // 2
    for ref, col in ((keys, 0), (values, kv_w)):
        whole = jnp.concatenate(
            [before[:WINDOW, col : col + kv_w], pair[:, col : col + kv_w], behind[:WINDOW, col : col + kv_w]], 0
        ).astype(jnp.float32)
        lane = lax.broadcasted_iota(jnp.int32, whole.shape, 1)
        turned = pltpu.roll(whole, HD, 1)
        zero = jnp.zeros_like(whole)
        ref[0] = jnp.where(lane < HD, whole, zero).astype(jnp.bfloat16)
        ref[1] = jnp.where(lane >= HD, turned, zero).astype(jnp.bfloat16)
        ref[2] = jnp.where(lane < HD, turned, zero).astype(jnp.bfloat16)
        ref[3] = jnp.where(lane >= HD, whole, zero).astype(jnp.bfloat16)
    pairs = query.shape[1] // lanes
    per_kv = pairs // 2

    def body(i, carry):
        start = pl.multiple_of(i * block, block)
        q_at = lax.broadcasted_iota(jnp.int32, (block, span), 0)
        k_at = lax.broadcasted_iota(jnp.int32, (block, span), 1)
        position = idx[1] + start - WINDOW + k_at
        gap = k_at - q_at
        valid = (gap >= 0) & (gap <= 2 * WINDOW) & (position >= 0) & (position < seq_total)
        lane = lax.broadcasted_iota(jnp.int32, (block, lanes), 1)
        tops = jnp.zeros((block, lanes), jnp.float32)
        for kv in range(2):
            for p in range(per_kv):
                at = kv * per_kv + p
                q = query[pl.ds(start, block), at * lanes : (at + 1) * lanes]
                mixed = jnp.zeros((block, lanes), jnp.float32)
                shares = []
                for side in range(2):
                    k = keys[2 * kv + side, pl.ds(start, span), :]
                    v = values[2 * kv + side, pl.ds(start, span), :]
                    scores = lax.dot_general(q, k, (((1,), (1,)), ((), ())), preferred_element_type=jnp.float32)
                    scores = jnp.where(valid, scores * HD ** (-0.5), neg_fill)
                    head = 2 * at + side
                    floor = sink[head]
                    top = jnp.maximum(jnp.max(scores, -1, keepdims=True), floor)
                    exps = jnp.exp(scores - top)
                    total = jnp.sum(exps, -1, keepdims=True) + jnp.exp(floor - top)
                    mixed += jnp.dot(exps.astype(jnp.bfloat16), v, preferred_element_type=jnp.float32)
                    shares.append(total)
                    tops = jnp.where(lane == head, top + jnp.log(total), tops)
                total = jnp.where(lane < HD, shares[0], shares[1])
                out[pl.ds(start, block), at * lanes : (at + 1) * lanes] = (mixed / total).astype(jnp.bfloat16)
        logs[:, pl.ds(start, block)] = tops.T[: logs.shape[0], :]
        return carry

    lax.fori_loop(0, rows // block, body, 0)


def attend(idx, query, pair, before, behind, sink, seq_total):
    rows = query.shape[0]
    wide = pair.shape[1] // 2
    return pl.pallas_call(
        functools.partial(attend_kernel, seq_total),
        out_shape=[
            jax.ShapeDtypeStruct(query.shape, jnp.bfloat16),
            jax.ShapeDtypeStruct((query.shape[1] // HD, rows), jnp.float32),
        ],
        in_specs=[SMEM] + [VMEM] * 4 + [SMEM],
        out_specs=[VMEM] * 2,
        scratch_shapes=[pltpu.VMEM((4, rows + 2 * WINDOW, wide), jnp.bfloat16)] * 2,
        name="attend",
    )(idx, query, pair, before, behind, sink)


def early_kernel(idx, pooled, attended, *refs):
    near, far, d1, s1, ed1, es1, d2, s2, ed2, es2 = refs[:10]
    outs, buf, sems = refs[10:14], refs[14], refs[15]
    core = idx[0]
    slots = [[(None, ref)] for ref in (near, far, d1, s1, ed1, es1)]
    slots += [[(core == 0, a), (core == 1, b)] for a, b in ((d2, ed2), (es2, s2))]
    fetch(slots, buf, sems)
    cut = pooled.shape[1]
    half = buf.shape[2]
    for i in range(8):
        arrived(slots, buf, sems, i)
        place = idx[1 + i]

        @pl.when(place >= 0)
        def _():
            part = jnp.dot(pooled[...], buf[i, :cut, :], preferred_element_type=jnp.float32)
            part += jnp.dot(attended[...], buf[i, cut:, :], preferred_element_type=jnp.float32)
            part = part.astype(jnp.bfloat16)
            col = pl.multiple_of((place % 2) * half, half)
            for r in range(4):

                @pl.when(place // 2 == r)
                def _():
                    outs[r][:, pl.ds(col, half)] = part


def out_early(idx, pooled, attended, slots):
    rows = pooled.shape[0]
    deep, wide = slots[0].shape
    return pl.pallas_call(
        early_kernel,
        out_shape=[jax.ShapeDtypeStruct((rows, 2 * wide), jnp.bfloat16)] * 4,
        in_specs=[SMEM] + [VMEM] * 2 + [ANY] * 10,
        out_specs=[VMEM] * 4,
        scratch_shapes=[pltpu.VMEM((8, deep, wide), jnp.bfloat16), pltpu.SemaphoreType.DMA((8,))],
        name="out_early",
    )(idx, pooled, attended, *slots)


def late_kernel(idx, pooled, attended, *refs):
    d2, s2, ed2, es2, d3, s3, ed3, es3, out, buf, sems = refs
    core, outer = idx[0], idx[1]
    slots = []
    for (a, b), (e, f) in (((d2, ed2), (d3, ed3)), ((es2, s2), (es3, s3))):
        slots.append(
            [
                ((outer == 0) & (core == 0), a),
                ((outer == 0) & (core == 1), b),
                ((outer == 1) & (core == 0), e),
                ((outer == 1) & (core == 1), f),
            ]
        )
    fetch(slots, buf, sems)
    cut = pooled.shape[1]
    half = buf.shape[2]
    for i in range(2):
        arrived(slots, buf, sems, i)
        part = jnp.dot(pooled[...], buf[i, :cut, :], preferred_element_type=jnp.float32)
        part += jnp.dot(attended[...], buf[i, cut:, :], preferred_element_type=jnp.float32)
        col = pl.multiple_of(idx[2 + i] * half, half)
        out[:, pl.ds(col, half)] = part.astype(jnp.bfloat16)


def out_late(idx, pooled, attended, slots):
    rows = pooled.shape[0]
    deep, wide = slots[0].shape
    return pl.pallas_call(
        late_kernel,
        out_shape=jax.ShapeDtypeStruct((rows, 2 * wide), jnp.bfloat16),
        in_specs=[SMEM] + [VMEM] * 2 + [ANY] * 8,
        out_specs=VMEM,
        scratch_shapes=[pltpu.VMEM((2, deep, wide), jnp.bfloat16), pltpu.SemaphoreType.DMA((2,))],
        name="out_late",
    )(idx, pooled, attended, *slots)


def sum_kernel(idx, *refs):
    early, late, own_early, own_late, out, buf, sems = refs[:4], refs[4:8], refs[8], refs[9], *refs[10:]
    is_late, has_own, own_round = idx[0], idx[1], idx[2]
    slots = []
    for r in range(4):
        mine = (has_own == 1) & (own_round == r)
        slots.append(
            [
                ((is_late == 0) & jnp.logical_not(mine), early[r]),
                ((is_late == 0) & mine, own_early),
                ((is_late == 1) & jnp.logical_not(mine), late[r]),
                ((is_late == 1) & mine, own_late),
            ]
        )
    fetch(slots, buf, sems)
    for r in range(4):
        arrived(slots, buf, sems, r)
    total = buf[0].astype(jnp.float32)
    for r in range(1, 4):
        total = total + buf[r].astype(jnp.float32)
    out[...] = total.astype(jnp.bfloat16)


def sum_parts(idx, early, late, own_early, own_late):
    shape = own_late.shape
    return pl.pallas_call(
        sum_kernel,
        out_shape=jax.ShapeDtypeStruct(shape, jnp.bfloat16),
        in_specs=[SMEM] + [ANY] * 10,
        out_specs=VMEM,
        scratch_shapes=[pltpu.VMEM((4, *shape), jnp.bfloat16), pltpu.SemaphoreType.DMA((4,))],
        name="sum",
    )(idx, *early, *late, own_early, own_late)


def line_gather(name, near, far):
    d1 = send(name + "_d1", near, line_one)
    s1 = send(name + "_s1", far, line_one)
    d2 = send(name + "_d2", d1, line_two(0))
    s2 = send(name + "_s2", s1, line_two(1))
    d3 = send(name + "_d3", d2, line_three(0))
    s3 = send(name + "_s3", s2, line_three(1))
    ed1 = send(name + "_ed1", d1, other_core)
    es1 = send(name + "_es1", s1, other_core)
    ed2 = send(name + "_ed2", d2, from_core(0))
    es2 = send(name + "_es2", s2, from_core(1))
    ed3 = send(name + "_ed3", d3, end_core(0))
    es3 = send(name + "_es3", s3, end_core(1))
    return (near, far, d1, s1, ed1, es1), (d2, s2, ed2, es2), (d3, s3, ed3, es3)


def turn_tables(positions):
    cos_r, sin_r, cos_c, sin_c = rope_tables(positions, HD)
    cosine = jnp.concatenate([cos_r, cos_r, cos_c, cos_c] * 2, 1)
    sine = jnp.concatenate([-sin_r, sin_r, -sin_c, sin_c] * 2, 1)
    return cosine, sine


def ints(*values):
    return jnp.stack([jnp.asarray(v, jnp.int32) for v in values])


def local_lines(
    tokens,
    norm_gain,
    query_weight,
    key_weight,
    value_weight,
    pool_in_weight,
    pool_mix_weight,
    sink_logit,
    out_pool_weight,
    out_attn_weight,
):
    s, t = lax.axis_index("sp"), lax.axis_index("tp")
    z, y, x, c = s // 2, s % 2, t // 2, t % 2
    home = y == c
    planes = lax.axis_size("sp") // 2
    tok_rows = tokens.shape[0]
    seq_total = tok_rows * lax.axis_size("sp")
    offset = (2 * z + c) * tok_rows
    group = 2 * x + y
    outer = (z == 0) | (z == planes - 1)

    w_in = pack("pack_in", (query_weight, key_weight, value_weight, pool_in_weight), 1)
    in_swapped = send("in_swap", w_in, swap_away)
    near = jnp.where(home, w_in, send("in_near", w_in, home_to_away))
    far = jnp.where(home, send("in_far", in_swapped, away_to_home), in_swapped)
    in_near, in_two, in_three = line_gather("in", near, far)

    p1 = send("tok1", tokens, token_one)
    p2 = send("tok2", tokens, token_two)
    p3 = send("tok3", tokens, away_to_home)
    p4 = send("tok4", p1, token_diag)
    p5 = send("tok5", p2, token_diag)

    w_out = pack("pack_out", (out_pool_weight, out_attn_weight), 0)
    out_swapped = send("out_swap", w_out, swap_away)
    mix_other = send("mix_swap", pool_mix_weight[0], swap_away)
    sink_other = send("sink_swap", sink_logit, swap_away)
    mix = jnp.where(home, pool_mix_weight[0], mix_other)
    sink = jnp.where(home, sink_logit, sink_other)
    o_near = jnp.where(home, w_out, send("out_near", w_out, home_to_away))
    o_far = jnp.where(home, send("out_far", out_swapped, away_to_home), out_swapped)
    out_near, out_two, out_three = line_gather("out", o_near, o_far)

    zr = jnp.where(c == 0, z - 1, z + 1)
    ze = jnp.where(c == 0, z + 1, z - 1)
    z2 = jnp.where(z < planes // 2, z + 2, z - 2)
    z3 = planes - 1 - z
    has_r = (zr >= 0) & (zr < planes)
    has_e = (ze >= 0) & (ze < planes)

    head = ints(home, 2 * x + c, 2 * x + 1 - c, 2 * (1 - x) + c, 2 * (1 - x) + 1 - c)
    normed = norm_tokens(head, (tokens, p1, p2, p3, p4, p5), norm_gain[None, :])

    near_idx = ints(
        2 * z + y,
        2 * z + 1 - y,
        jnp.where(has_r, 2 * zr + y, -1),
        jnp.where(has_r, 2 * zr + 1 - y, -1),
        jnp.where(has_e, 2 * ze + y, -1),
        jnp.where(has_e, 2 * ze + 1 - y, -1),
    )
    acc = project_near(near_idx, normed, in_near)
    far_idx = ints(c, 2 * z2 + y, 2 * z2 + 1 - y, 2 * z3 + y, 2 * z3 + 1 - y)
    widths = (query_weight.shape[1], key_weight.shape[1])
    tables = turn_tables(offset + jnp.arange(tok_rows, dtype=jnp.int32))
    query, pair, pool_input, low, high = project_far(far_idx, normed, acc, tables, in_two + in_three, widths)

    before = send("halo_next", high, halo_next)
    behind = send("halo_prev", low, halo_prev)
    place = ints(group, offset)
    pool_out = pool_mixer(place, pool_input, before, behind, mix, seq_total)
    attended, log_here = attend(place, query, pair, before, behind, sink, seq_total)
    log_weight = jnp.where(home, log_here, send("log_swap", log_here, swap_away))

    def slot(zz, parity, ok):
        return jnp.where(ok, 2 * (zz ^ group) + parity, -1)

    early_idx = ints(
        c,
        slot(z, y, True),
        slot(z, 1 - y, True),
        slot(zr, y, has_r),
        slot(zr, 1 - y, has_r),
        slot(ze, y, has_e),
        slot(ze, 1 - y, has_e),
        slot(z2, y, outer),
        slot(z2, 1 - y, outer),
    )
    blocks = out_early(early_idx, pool_out, attended, out_near + out_two)
    late = out_late(ints(c, outer, y, 1 - y), pool_out, attended, out_two + out_three)
    early_parts = [send(f"early{r}", blocks[r], part_early(r)) for r in range(4)]
    late_parts = [send(f"late{r}", late, part_late(r)) for r in range(4)]
    last = jnp.where(z < planes // 2, planes - 1, 0)
    mixed = sum_parts(ints(t == last, home, 0), early_parts, late_parts, blocks[0], late)
    return (mixed, log_weight)


def solution(mesh):
    lines = mesh.shape["sp"] == 8 and mesh.shape["tp"] == 4
    return jax.shard_map(
        local_lines if lines else local,
        mesh=mesh,
        in_specs=(
            P("sp", "tp"),
            P(),
            P("sp", "tp"),
            P("sp", "tp"),
            P("sp", "tp"),
            P("sp", "tp"),
            P("tp", None, None),
            P("tp"),
            P("tp", "sp"),
            P("tp", "sp"),
        ),
        out_specs=(P("sp", "tp"), P("tp", "sp")),
        check_vma=False,
    )
```

```python
import functools

import jax
import jax.numpy as jnp
from jax import lax
from jax.experimental import pallas as pl
from jax.experimental.pallas import tpu as pltpu
from jax.sharding import PartitionSpec as P


HD = 64
WINDOW = 128
GRID_W = 64


norm_eps = 1e-06
rope_base = 10000.0
pool_reach = 8
neg_fill = -1e30


def with_halo(cells, sides, width):
    for axis, dim in sides:
        count = lax.axis_size(axis)
        ends = count - 1
        head = lax.slice_in_dim(cells, 0, width, axis=dim)
        tail = lax.slice_in_dim(cells, cells.shape[dim] - width, cells.shape[dim], axis=dim)
        cells = jnp.concatenate(
            [
                lax.ppermute(tail, axis, [(i, (i + 1) % count) for i in range(ends)]),
                cells,
                lax.ppermute(head, axis, [((i + 1) % count, i) for i in range(ends)]),
            ],
            axis=dim,
        )
    return cells


def rope_tables(positions, head_dim):
    n_freq = head_dim // 4
    freqs = rope_base ** (-jnp.arange(n_freq, dtype=jnp.float32) / n_freq)
    rows = (positions // GRID_W).astype(jnp.float32)
    columns = (positions % GRID_W).astype(jnp.float32)
    row_angle = rows[:, None] * freqs[None, :]
    col_angle = columns[:, None] * freqs[None, :]
    return (jnp.cos(row_angle), jnp.sin(row_angle), jnp.cos(col_angle), jnp.sin(col_angle))


def rotate_half(values, cosine, sine):
    middle = values.shape[-1] // 2
    first = values[..., :middle]
    second = values[..., middle:]
    return jnp.concatenate([first * cosine - second * sine, second * cosine + first * sine], -1)


def rotate_heads(values, tables, head_dim):
    rows_count = values.shape[0]
    shaped = values.astype(jnp.float32).reshape(rows_count, -1, head_dim)
    cos_r, sin_r, cos_c, sin_c = [table[:, None, :] for table in tables]
    split = head_dim // 2
    turned = jnp.concatenate(
        [
            rotate_half(shaped[..., :split], cos_r, sin_r),
            rotate_half(shaped[..., split:], cos_c, sin_c),
        ],
        -1,
    )
    return turned.reshape(rows_count, -1).astype(jnp.bfloat16)


def pool_group(extended, own, positions, half_width, seq_total):
    rows_count = own.shape[0]
    summed = jnp.zeros(own.shape, jnp.float32)
    counted = jnp.zeros((rows_count,), jnp.float32)
    for shift_by in range(-pool_reach, pool_reach):
        source = positions + shift_by
        inside = (
            (shift_by >= -half_width)
            & (shift_by < half_width)
            & (source >= 0)
            & (source < seq_total)
        )
        window_rows = extended[pool_reach + shift_by : pool_reach + shift_by + rows_count].astype(
            jnp.float32
        )
        summed = summed + jnp.where(inside[:, None], window_rows, 0.0)
        counted = counted + inside.astype(jnp.float32)
    return (summed / counted[:, None] - own.astype(jnp.float32)).astype(jnp.bfloat16)


def attend_block(queries, keys, values, sink, query_pos, key_pos, seq_total):
    scores = jnp.einsum(
        "qhgd,khd->hgqk", queries, keys, preferred_element_type=jnp.float32
    ) * HD ** (-0.5)
    valid = (
        (jnp.abs(query_pos[:, None] - key_pos[None, :]) <= WINDOW)
        & (key_pos >= 0)[None, :]
        & (key_pos < seq_total)[None, :]
    )
    scores = jnp.where(valid, scores, neg_fill)
    row_top = jnp.maximum(jnp.max(scores, -1), sink[:, :, None])
    exps = jnp.exp(scores - row_top[..., None])
    row_total = jnp.sum(exps, -1) + jnp.exp(sink[:, :, None] - row_top)
    weights = (exps / row_total[..., None]).astype(jnp.bfloat16)
    attended = jnp.einsum("hgqk,khd->qhgd", weights, values, preferred_element_type=jnp.float32)
    return (attended.astype(jnp.bfloat16), row_top + jnp.log(row_total))


def attend_all(rot_query, key_ext, value_ext, sink_logit, offset, seq_total):
    tok_rows = rot_query.shape[0]
    heads_local = rot_query.shape[1] // HD
    kv_local = key_ext.shape[1] // HD
    grp = heads_local // kv_local
    query_heads = rot_query.reshape(tok_rows, kv_local, grp, HD)
    key_heads = key_ext.reshape(-1, kv_local, HD)
    value_heads = value_ext.reshape(-1, kv_local, HD)
    sink = sink_logit.reshape(kv_local, grp)
    block_rows = min(tok_rows, 256)
    attended_parts = []
    log_parts = []
    for block_index in range(tok_rows // block_rows):
        start = block_index * block_rows
        query_pos = offset + start + jnp.arange(block_rows, dtype=jnp.int32)
        key_pos = offset + start - WINDOW + jnp.arange(block_rows + 2 * WINDOW, dtype=jnp.int32)
        attended_block, log_block = attend_block(
            query_heads[start : start + block_rows],
            key_heads[start : start + block_rows + 2 * WINDOW],
            value_heads[start : start + block_rows + 2 * WINDOW],
            sink,
            query_pos,
            key_pos,
            seq_total,
        )
        attended_parts.append(attended_block.reshape(block_rows, heads_local * HD))
        log_parts.append(log_block.reshape(heads_local, block_rows))
    attended = jnp.concatenate(attended_parts, 0)
    log_weight = jnp.concatenate(log_parts, 1)
    return (attended, log_weight)


def fetch_outputs(out_pool_weight, out_attn_weight):
    return (
        lax.all_gather(out_pool_weight, "sp", axis=1, tiled=True),
        lax.all_gather(out_attn_weight, "sp", axis=1, tiled=True),
    )


def local(
    tokens,
    norm_gain,
    query_weight,
    key_weight,
    value_weight,
    pool_in_weight,
    pool_mix_weight,
    sink_logit,
    out_pool_weight,
    out_attn_weight,
):
    whole = lax.all_gather(tokens, "tp", axis=1, tiled=True)
    wide = whole.astype(jnp.float32)
    normed = (
        wide * lax.rsqrt(jnp.mean(wide * wide, -1, keepdims=True) + norm_eps) * norm_gain
    ).astype(jnp.bfloat16)
    tok_rows = normed.shape[0]
    seq_total = tok_rows * lax.axis_size("sp")
    offset = lax.axis_index("sp") * tok_rows
    weights_in = (query_weight, key_weight, value_weight, pool_in_weight)
    pieces = (
        lax.all_gather(weights_in[0], "sp", axis=0, tiled=True),
        lax.all_gather(weights_in[1], "sp", axis=0, tiled=True),
        lax.all_gather(weights_in[2], "sp", axis=0, tiled=True),
        lax.all_gather(weights_in[3], "sp", axis=0, tiled=True),
    )
    sums = tuple((jnp.dot(normed, piece, preferred_element_type=jnp.float32) for piece in pieces))
    query, key, value, pool_input = [total.astype(jnp.bfloat16) for total in sums]
    positions = offset + jnp.arange(tok_rows, dtype=jnp.int32)
    tables = rope_tables(positions, HD)
    rot_query = rotate_heads(query, tables, HD)
    rot_key = rotate_heads(key, tables, HD)
    key_width = rot_key.shape[1]
    pool_ext = with_halo(pool_input, (("sp", 0),), pool_reach)
    pair_ext = with_halo(jnp.concatenate([rot_key, value], 1), (("sp", 0),), WINDOW)
    key_ext = pair_ext[:, :key_width]
    value_ext = pair_ext[:, key_width:]
    half_width = jnp.left_shift(jnp.int32(1), lax.axis_index("tp"))
    pooled = pool_group(pool_ext, pool_input, positions, half_width, seq_total)
    pool_out = jnp.dot(pooled, pool_mix_weight[0], preferred_element_type=jnp.float32).astype(
        jnp.bfloat16
    )
    attended, log_weight = attend_all(rot_query, key_ext, value_ext, sink_logit, offset, seq_total)
    out_pool_full, out_attn_full = fetch_outputs(out_pool_weight, out_attn_weight)
    term = jnp.dot(pool_out, out_pool_full, preferred_element_type=jnp.float32)
    term = term + jnp.dot(attended, out_attn_full, preferred_element_type=jnp.float32)
    mixed = lax.psum_scatter(term.astype(jnp.bfloat16), "tp", scatter_dimension=1, tiled=True)
    return (mixed, log_weight)


ANY = pl.BlockSpec(memory_space=pl.ANY)
HBM = pl.BlockSpec(memory_space=pltpu.HBM)
SMEM = pl.BlockSpec(memory_space=pltpu.SMEM)
VMEM = pl.BlockSpec(memory_space=pltpu.VMEM)


def lin(z, y, x, c):
    return ((z * 2 + y) * 2 + x) * 2 + c


def make_perm(rule):
    pairs = []
    for z in range(4):
        for y in range(2):
            for x in range(2):
                for c in range(2):
                    to = rule(z, y, x, c)
                    if to is not None and to != (z, y, x, c):
                        pairs.append((lin(z, y, x, c), lin(*to)))
    return pairs


def send(value, rule):
    return lax.ppermute(value, ("sp", "tp"), make_perm(rule))


def swap_away(z, y, x, c):
    return (z, c, x, y) if y != c else None


def other_core(z, y, x, c):
    return (z, y, x, 1 - c)


def flip_x(z, y, x, c):
    return (z, y, 1 - x, c)


def flip_y(z, y, x, c):
    return (z, 1 - y, x, c)


def flip_xy(z, y, x, c):
    return (z, 1 - y, 1 - x, c)


def plane_two(z, y, x, c):
    return (z ^ 2, y, x, c)


def plane_pair(z, y, x, c):
    return (z ^ 1, y, x, c)


def plane_mid(z, y, x, c):
    return (3 - z, y, x, c) if z in (1, 2) else None


def plane_end(z, y, x, c):
    return (z ^ 1, y, x, c) if z in (1, 2) else None


def across_planes(z, y, x, c):
    to = z + 1 if c == 1 else z - 1
    return (to, y, x, 1 - c) if 0 <= to <= 3 else None


def late_core(z):
    return 1 - z % 2


def give_early(z, y, x, c):
    return (z, y, x, 1 - c) if c == late_core(z) else None


def give_late(z, y, x, c):
    return (z, y, x, 1 - c) if c != late_core(z) else None


def position():
    s, t = lax.axis_index("sp"), lax.axis_index("tp")
    return s // 2, s % 2, t // 2, t % 2


def call(kernel, args, specs, outs, out_specs, scratch=(), vmem=None):
    params = {} if vmem is None else {"compiler_params": pltpu.CompilerParams(vmem_limit_bytes=vmem << 20)}
    return pl.pallas_call(
        kernel, out_shape=outs, in_specs=specs, out_specs=out_specs, scratch_shapes=list(scratch), **params
    )(*args)


def shape_of(shape, dtype=jnp.bfloat16):
    return jax.ShapeDtypeStruct(shape, dtype)


def pack_kernel(axis, *refs):
    sources, out, sems = refs[:-2], refs[-2], refs[-1]
    copies = []
    at = 0
    for i, source in enumerate(sources):
        size = source.shape[axis]
        span = pl.ds(at, size)
        where = (span, slice(None)) if axis == 0 else (slice(None), span)
        copies.append(pltpu.make_async_copy(source, out.at[where], sems.at[i]))
        copies[-1].start()
        at += size
    for copy in copies:
        copy.wait()


def pack(arrays, axis):
    shape = list(arrays[0].shape)
    shape[axis] = sum(a.shape[axis] for a in arrays)
    return call(
        functools.partial(pack_kernel, axis),
        arrays,
        [HBM] * len(arrays),
        shape_of(tuple(shape), arrays[0].dtype),
        VMEM,
        [pltpu.SemaphoreType.DMA((len(arrays),))],
        4,
    )


def dma_sems(count):
    return pltpu.SemaphoreType.DMA((count,))


def choose_kernel(axis, count, *refs):
    _, y, _, c = position()
    own, sent, out, sems = refs[:count], refs[count : 2 * count], refs[-2], refs[-1]
    at = 0
    waits = []
    for i in range(count):
        size = out.shape[axis] - at if i == count - 1 else own[i].shape[axis]
        span = pl.ds(at, size)
        to = out.at[(span, slice(None)) if axis == 0 else (slice(None), span)]
        for when, ref in ((y == c, own[i]), (y != c, sent[i])):
            part = ref if ref.shape == to.shape else ref.at[pl.ds(0, to.shape[0]), :]
            pl.when(when)(pltpu.make_async_copy(part, to, sems.at[i]).start)
        waits.append(pltpu.make_async_copy(to, to, sems.at[i]))
        at += size
    for wait in waits:
        wait.wait()


def choose(own, sent, axis, shape):
    kernel = functools.partial(choose_kernel, axis, len(own))
    return call(kernel, (*own, *sent), [ANY] * (2 * len(own)), shape_of(shape), VMEM, [dma_sems(len(own))], 4)


def fetch(slots, buf, sems):
    for i, choices in enumerate(slots):
        for when, ref in choices:
            copy = pltpu.make_async_copy(ref, buf.at[i], sems.at[i])
            if when is None:
                copy.start()
            else:
                pl.when(when)(copy.start)


def arrived(slots, buf, sems, i):
    pltpu.make_async_copy(slots[i][0][1], buf.at[i], sems.at[i]).wait()


def load_pieces(pieces, buf, sems):
    _, y, x, _ = position()
    places = (2 * y + x, 2 * y + 1 - x, 2 * (1 - y) + x, 2 * (1 - y) + 1 - x)
    copies = [pltpu.make_async_copy(ref, buf.at[at], sems.at[i]) for i, (ref, at) in enumerate(zip(pieces, places))]
    for copy in copies:
        copy.start()
    for copy in copies:
        copy.wait()


def stats_kernel(own, px, py, pxy, stats, buf, sems):
    load_pieces((own, px, py, pxy), buf, sems)
    rows, wide = buf.shape[1:]
    step = 64

    def body(i, carry):
        at = pl.ds(pl.multiple_of(i * step, step), step)
        for token in range(2):
            total = jnp.zeros((step, wide), jnp.float32)
            for xx in range(2):
                v = buf[2 * token + xx, at, :].astype(jnp.float32)
                total = total + v * v
            stats[token, at, :] = jnp.broadcast_to(jnp.sum(total, -1, keepdims=True), (step, stats.shape[2]))
        return carry

    lax.fori_loop(0, rows // step, body, 0)


def row_stats(pieces):
    rows, wide = pieces[0].shape
    scratch = [pltpu.VMEM((4, rows, wide), jnp.bfloat16), dma_sems(4)]
    return call(stats_kernel, pieces, [ANY] * 4, shape_of((2, rows, 128), jnp.float32), VMEM, scratch, 8)


def prep_kernel(own, px, py, pxy, stats, stats_other, gain, keep, give, buf, sems):
    _, _, _, c = position()
    load_pieces((own, px, py, pxy), buf, sems)
    rows, wide = buf.shape[1:]
    half = wide // 2
    step = 64
    mine = pl.multiple_of(c * half, half)
    theirs = pl.multiple_of((1 - c) * half, half)

    def body(i, carry):
        at = pl.ds(pl.multiple_of(i * step, step), step)
        for token in range(2):
            total = stats[token, at, :] + stats_other[token, at, :]
            scale = lax.rsqrt(total / (4 * wide) + norm_eps)
            scale = jnp.concatenate([scale] * (half // scale.shape[1]), 1)
            for xx in range(2):
                for ref, start in ((keep, mine), (give, theirs)):
                    v = buf[2 * token + xx, at, pl.ds(start, half)].astype(jnp.float32)
                    factor = gain[:, pl.ds(pl.multiple_of((2 * xx + c) * wide + start, half), half)]
                    ref[2 * token + xx, at, :] = (v * scale * factor).astype(jnp.bfloat16)
        return carry

    lax.fori_loop(0, rows // step, body, 0)


def prepare(pieces, stats, stats_other, gain):
    rows, wide = pieces[0].shape
    half = shape_of((4, rows, wide // 2))
    scratch = [pltpu.VMEM((4, rows, wide), jnp.bfloat16), dma_sems(4)]
    return call(prep_kernel, (*pieces, stats, stats_other, gain), [ANY] * 4 + [VMEM] * 3, [half] * 2, [VMEM] * 2, scratch, 16)


COLS = 256


def pick(keep, got, token, zz, c):
    return jnp.where(zz % 2 == c, keep[2 * token + zz // 2], got[2 * token + zz // 2])


def near_slots(cur, two):
    return [[(None, cur)], [(None, two)]]


def near_reached(z):
    return z, z ^ 2


def far_slots(z, planes, pair, mid, end):
    inner = (z > 0) & (z < planes - 1)
    return [[(None, pair)], [(inner, mid), (jnp.logical_not(inner), end)]]


def far_reached(z, planes):
    return z ^ 1, planes - 1 - z


def near_kernel(keep, got, cur, two, own_acc, other_acc, buf, sems):
    z, _, _, c = position()
    slots = near_slots(cur, two)
    fetch(slots, buf, sems)
    for i in range(2):
        arrived(slots, buf, sems, i)
    reached = near_reached(z)
    for acc, token in ((own_acc, c), (other_acc, 1 - c)):
        ins = [pick(keep, got, token, zz, c) for zz in reached]
        for col in range(0, acc.shape[1], COLS):
            span = slice(col, col + COLS)
            part = jnp.dot(ins[0], buf[0, :, span], preferred_element_type=jnp.float32)
            acc[:, span] = part + jnp.dot(ins[1], buf[1, :, span], preferred_element_type=jnp.float32)


def project_near(keep, got, cur, two):
    rows = keep.shape[1]
    deep, cols = cur.shape
    scratch = [pltpu.VMEM((2, deep, cols), jnp.bfloat16), dma_sems(2)]
    outs = [shape_of((rows, cols), jnp.float32)] * 2
    return call(near_kernel, (keep, got, cur, two), [VMEM] * 2 + [ANY] * 2, outs, [VMEM] * 2, scratch, 16)


def columns(slots, start, width):
    return [[(when, ref.at[:, pl.ds(start, width)]) for when, ref in choices] for choices in slots]


def other_kernel(start, keep, got, acc, near_pair, mid, end, out, buf, sems):
    z, _, _, c = position()
    planes = keep.shape[0]
    slots = columns(far_slots(z, planes, near_pair, mid, end), start, out.shape[1])
    fetch(slots, buf, sems)
    ins = [pick(keep, got, 1 - c, zz, c) for zz in far_reached(z, planes)]
    for i in range(2):
        arrived(slots, buf, sems, i)
    for col in range(0, out.shape[1], COLS):
        span = slice(col, col + COLS)
        part = acc[:, start + col : start + col + COLS]
        part = part + jnp.dot(ins[0], buf[0, :, span], preferred_element_type=jnp.float32)
        out[:, span] = part + jnp.dot(ins[1], buf[1, :, span], preferred_element_type=jnp.float32)


def project_other(start, width, keep, got, acc, far):
    deep = far[0].shape[0]
    scratch = [pltpu.VMEM((2, deep, width), jnp.bfloat16), dma_sems(2)]
    outs = shape_of((acc.shape[0], width), jnp.float32)
    kernel = functools.partial(other_kernel, start)
    return call(kernel, (keep, got, acc, *far), [VMEM] * 3 + [ANY] * 3, outs, VMEM, scratch, 12)


def table_kernel(freqs, signs, cosine, sine):
    z, _, _, c = position()
    rows, lanes = cosine.shape
    at = (2 * z + c) * rows + lax.broadcasted_iota(jnp.int32, (rows, lanes), 0)
    lane = lax.broadcasted_iota(jnp.int32, (rows, lanes), 1)
    which = jnp.where(lane % HD < HD // 2, at // GRID_W, at % GRID_W)
    angle = which.astype(jnp.float32) * freqs[...]
    cosine[...] = jnp.cos(angle)
    sine[...] = jnp.sin(angle) * signs[...]


def turn_tables(rows):
    quarter = HD // 4
    freqs = rope_base ** (-jnp.arange(quarter, dtype=jnp.float32) / quarter)
    freqs = jnp.tile(freqs, 8)[None, :]
    signs = jnp.tile(jnp.concatenate([-jnp.ones(quarter, jnp.float32), jnp.ones(quarter, jnp.float32)]), 4)[None, :]
    outs = [shape_of((rows, 2 * HD), jnp.float32)] * 2
    return call(table_kernel, (freqs, signs), [VMEM] * 2, outs, [VMEM] * 2, (), 4)


def turn(v, cosine, sine):
    lane = lax.broadcasted_iota(jnp.int32, v.shape, 1)
    quarter = HD // 4
    partner = jnp.where(lane % (2 * quarter) < quarter, pltpu.roll(v, v.shape[1] - quarter, 1), pltpu.roll(v, quarter, 1))
    return v * cosine + partner * sine


def own_columns(start, keep, got, acc, theirs, far, buf, other, sems):
    z, _, _, c = position()
    planes = keep.shape[0]
    arrival = pltpu.make_async_copy(theirs, other, sems.at[2])
    arrival.start()
    slots = columns(far_slots(z, planes, *far), start, other.shape[1])
    fetch(slots, buf, sems)
    ins = [pick(keep, got, c, zz, c) for zz in far_reached(z, planes)]
    for i in range(2):
        arrived(slots, buf, sems, i)
    arrival.wait()
    for col in range(0, other.shape[1], COLS):
        span = slice(col, col + COLS)
        total = acc[:, start + col : start + col + COLS] + other[:, span]
        for i in range(2):
            total += jnp.dot(ins[i], buf[i, :, span], preferred_element_type=jnp.float32)
        yield col, total.astype(jnp.bfloat16)


def query_kernel(start, keep, got, acc, cosine, sine, theirs, near_pair, mid, end, query, buf, other, sems):
    lanes = cosine.shape[1]
    for col, total in own_columns(start, keep, got, acc, theirs, (near_pair, mid, end), buf, other, sems):
        for sub in range(0, COLS, lanes):
            v = turn(total[:, sub : sub + lanes].astype(jnp.float32), cosine[...], sine[...])
            query[:, col + sub : col + sub + lanes] = (v * HD ** (-0.5)).astype(jnp.bfloat16)


def pair_kernel(start, keep, got, acc, cosine, sine, theirs, near_pair, mid, end, pair, pool, near, far, buf, other, sems):
    _, _, _, c = position()
    lanes = cosine.shape[1]
    rows = acc.shape[0]
    for col, total in own_columns(start, keep, got, acc, theirs, (near_pair, mid, end), buf, other, sems):
        if col == 0:
            pair[:, :lanes] = turn(total[:, :lanes].astype(jnp.float32), cosine[...], sine[...]).astype(jnp.bfloat16)
            pair[:, lanes:] = total[:, lanes:]
        else:
            pool[...] = total
    for first, edge, core in ((0, near, 1), (rows - WINDOW, near, 0), (0, far, 0), (rows - WINDOW, far, 1)):

        @pl.when(c == core)
        def _():
            edge[:WINDOW, :] = pair[first : first + WINDOW, :]
            row = 0 if first == 0 else rows - pool_reach
            edge[WINDOW:, :] = pool[row : row + pool_reach, :]


def project_own(kernel, start, keep, got, acc, tables, theirs, far, outs):
    deep = far[0].shape[0]
    width = theirs.shape[1]
    scratch = [pltpu.VMEM((2, deep, width), jnp.bfloat16), pltpu.VMEM(theirs.shape, jnp.float32), dma_sems(3)]
    outs = [shape_of(shape) for shape in outs]
    args = (keep, got, acc, *tables, theirs, *far)
    kernel = functools.partial(kernel, start)
    return call(kernel, args, [VMEM] * 5 + [ANY] * 4, outs, [VMEM] * len(outs), scratch, 16)


def mix_pool(z, y, x, c, seq_total, own, before, behind, matrix, out, ext):
    rows, wide = own.shape
    ext[:pool_reach, :] = before[WINDOW:, :].astype(jnp.float32)
    ext[pool_reach : pool_reach + rows, :] = own[...].astype(jnp.float32)
    ext[pool_reach + rows :, :] = behind[WINDOW:, :].astype(jnp.float32)
    at = (2 * z + c) * rows + lax.broadcasted_iota(jnp.int32, (rows, 1), 0)
    for g in range(4):

        @pl.when(2 * x + y == g)
        def _():
            reach = 1 << g
            total = ext[pool_reach - reach : pool_reach - reach + rows, :]
            for shift in range(1 - reach, reach):
                total = total + ext[pool_reach + shift : pool_reach + shift + rows, :]
            count = jnp.minimum(at + reach, seq_total) - jnp.maximum(at - reach, 0)
            mean = total / count.astype(jnp.float32)
            pooled = (mean - ext[pool_reach : pool_reach + rows, :]).astype(jnp.bfloat16)
            out[:, :wide] = jnp.dot(pooled, matrix, preferred_element_type=jnp.float32).astype(jnp.bfloat16)


def attend_kernel(seq_total, query, pair, pool, inside, outside, mix, swapped, sink, sink_other, out, logs, keys, values, ext):
    z, y, x, c = position()
    rows = query.shape[0]
    offset = (2 * z + c) * rows
    lanes = 2 * HD
    block = WINDOW
    span = 3 * block
    kv_w = pair.shape[1] // 2
    cut = out.shape[1] - query.shape[1]
    before = jnp.where(c == 0, outside[...], inside[...])
    behind = jnp.where(c == 0, inside[...], outside[...])
    matrix = jnp.where(y == c, mix[...], swapped[...])
    mix_pool(z, y, x, c, seq_total, pool, before, behind, matrix, out, ext)
    for ref, col in ((keys, 0), (values, kv_w)):
        whole = jnp.concatenate(
            [before[:WINDOW, col : col + kv_w], pair[:, col : col + kv_w], behind[:WINDOW, col : col + kv_w]], 0
        ).astype(jnp.float32)
        lane = lax.broadcasted_iota(jnp.int32, whole.shape, 1)
        turned = pltpu.roll(whole, HD, 1)
        ref[0, :, :lanes] = jnp.where(lane < HD, whole, 0.0).astype(jnp.bfloat16)
        ref[1, :, :lanes] = jnp.where(lane >= HD, turned, 0.0).astype(jnp.bfloat16)
        ref[2, :, :lanes] = jnp.where(lane < HD, turned, 0.0).astype(jnp.bfloat16)
        ref[3, :, :lanes] = jnp.where(lane >= HD, whole, 0.0).astype(jnp.bfloat16)
    lane = lax.broadcasted_iota(jnp.int32, values.shape[1:2] + (lanes,), 1)
    for side in range(2):
        ones = jnp.where((lane < HD) == (side == 0), 1.0, 0.0).astype(jnp.bfloat16)
        values[side, :, lanes:] = ones
        values[2 + side, :, lanes:] = ones

    def body(i, carry):
        start = pl.multiple_of(i * block, block)
        rows_at = pl.ds(start, block)
        q_at = lax.broadcasted_iota(jnp.int32, (block, block), 0)
        k_at = lax.broadcasted_iota(jnp.int32, (block, block), 1)
        first = jnp.where((k_at >= q_at) & (offset + start - WINDOW + k_at >= 0), 0.0, neg_fill)
        last = jnp.where((k_at <= q_at) & (offset + start + WINDOW + k_at < seq_total), 0.0, neg_fill)
        first2, last2 = jnp.concatenate([first, first], 0), jnp.concatenate([last, last], 0)
        lane = lax.broadcasted_iota(jnp.int32, (2 * block, lanes), 1)
        even = lane < HD
        upper = lax.broadcasted_iota(jnp.int32, (2 * block, lanes), 0) < block
        slim = lax.broadcasted_iota(jnp.int32, (block, lanes), 1)
        tops = jnp.zeros((block, lanes), jnp.float32)
        for kv in range(2):
            base = 2 * kv * lanes
            q = jnp.concatenate([query[rows_at, base : base + lanes], query[rows_at, base + lanes : base + 2 * lanes]], 0)
            k = jnp.concatenate([keys[2 * kv + side, pl.ds(start, span), :] for side in range(2)], 0)
            v = jnp.concatenate([values[2 * kv + side, pl.ds(start, span), :] for side in range(2)], 0)
            scores = lax.dot_general(q, k, (((1,), (1,)), ((), ())), preferred_element_type=jnp.float32)
            exps, peaks, floors = [], [], []
            for side in range(2):
                col = side * span
                s0 = scores[:, col : col + block] + first2
                s1 = scores[:, col + block : col + 2 * block]
                s2 = scores[:, col + 2 * block : col + span] + last2
                heads = [4 * kv + 2 * p + side for p in range(2)]
                sinks = [jnp.where(y == c, sink[head], sink_other[head]) for head in heads]
                floor = jnp.where(upper, sinks[0], sinks[1])
                top = jnp.max(jnp.maximum(jnp.maximum(jnp.maximum(s0, s1), s2), floor), -1, keepdims=True)
                exps += [jnp.exp(part - top).astype(jnp.bfloat16) for part in (s0, s1, s2)]
                peaks.append(top)
                floors.append(floor)
            both = jnp.dot(jnp.concatenate(exps, 1), v, preferred_element_type=jnp.float32)
            top = jnp.where(even, peaks[0], peaks[1])
            total = both[:, lanes:] + jnp.exp(jnp.where(even, floors[0], floors[1]) - top)
            done = (both[:, :lanes] / total).astype(jnp.bfloat16)
            logged = top + jnp.log(total)
            for p in range(2):
                out[rows_at, cut + base + p * lanes : cut + base + (p + 1) * lanes] = done[p * block : (p + 1) * block]
                head = 4 * kv + 2 * p
                tops = jnp.where((slim == head) | (slim == HD + head + 1), logged[p * block : (p + 1) * block], tops)
        turned = tops.T
        for head in range(logs.shape[0]):
            row = head + HD * (head % 2)
            logs[head : head + 1, rows_at] = turned[row : row + 1, :]
        return carry

    lax.fori_loop(0, rows // block, body, 0)


def attend(query, pair, pool, inside, outside, mix, swapped, sink, sink_other, seq_total):
    rows = query.shape[0]
    wide = pair.shape[1] // 2
    long = rows + 2 * WINDOW
    outs = [shape_of((rows, query.shape[1] + pool.shape[1])), shape_of((query.shape[1] // HD, rows), jnp.float32)]
    scratch = [
        pltpu.VMEM((4, long, wide), jnp.bfloat16),
        pltpu.VMEM((4, long, 2 * wide), jnp.bfloat16),
        pltpu.VMEM((rows + 2 * pool_reach, pool.shape[1]), jnp.float32),
    ]
    kernel = functools.partial(attend_kernel, seq_total)
    args = (query, pair, pool, inside, outside, mix, swapped, sink, sink_other)
    return call(kernel, args, [VMEM] * 7 + [SMEM] * 2, outs, [VMEM] * 2, scratch, 20)


def out_kernel(late, acts, acts_other, *refs):
    pieces, outs, (buf, blocks, sems) = refs[:-7], refs[-7:-3], refs[-3:]
    z, y, x, c = position()
    planes = len(outs)
    if late:
        slots, reached = far_slots(z, planes, *pieces), far_reached(z, planes)
    else:
        slots, reached = near_slots(*pieces), near_reached(z)
    fetch(slots, buf, sems)
    for i in range(2):
        arrived(slots, buf, sems, i)
        across = (reached[i] // 2) ^ x
        for tokens, theirs in ((acts, 0), (acts_other, 1)):
            part = jnp.dot(tokens[...], buf[i], preferred_element_type=jnp.float32)
            blocks[2 * (c ^ y ^ theirs) + across] = part.astype(jnp.bfloat16)
    copies = [pltpu.make_async_copy(blocks.at[r], outs[r], sems.at[2 + r]) for r in range(4)]
    for copy in copies:
        copy.start()
    for copy in copies:
        copy.wait()


def out_blocks(late, acts, acts_other, pieces):
    rows = acts.shape[0]
    deep, wide = pieces[0].shape
    scratch = [pltpu.VMEM((2, deep, wide), jnp.bfloat16), pltpu.VMEM((4, rows, wide), jnp.bfloat16), dma_sems(6)]
    outs = [shape_of((rows, wide))] * 4
    kernel = functools.partial(out_kernel, late)
    return call(kernel, (acts, acts_other, *pieces), [VMEM] * 2 + [ANY] * len(pieces), outs, [ANY] * 4, scratch, 12)


def sum_kernel(a, b, e, d, out):
    total = a[...].astype(jnp.float32) + b[...].astype(jnp.float32) + e[...].astype(jnp.float32) + d[...].astype(jnp.float32)
    out[...] = total.astype(jnp.bfloat16)


def sum_parts(parts):
    return call(sum_kernel, parts, [VMEM] * 4, shape_of(parts[0].shape), VMEM, (), 8)


def last_kernel(early, late, early_other, late_other, out, sems):
    z, _, _, c = position()
    half = early.shape[1]
    mine = c == 1 - z % 2
    at = pl.ds(pl.multiple_of(c * half, half), half)
    over = pl.ds(pl.multiple_of((1 - c) * half, half), half)
    for keep, got, when in ((late, late_other, mine), (early, early_other, jnp.logical_not(mine))):

        @pl.when(when)
        def _():
            pltpu.make_async_copy(keep, out.at[:, at], sems.at[0]).start()
            pltpu.make_async_copy(got, out.at[:, over], sems.at[1]).start()

    pltpu.make_async_copy(late, out.at[:, at], sems.at[0]).wait()
    pltpu.make_async_copy(late, out.at[:, over], sems.at[1]).wait()


def assemble(early, late, early_other, late_other):
    rows, half = early.shape
    return call(last_kernel, (early, late, early_other, late_other), [ANY] * 4, shape_of((rows, 2 * half)), VMEM, [dma_sems(2)], 4)


def line_gather(cur):
    two = send(cur, plane_two)
    pair = send(cur, plane_pair)
    mid = send(cur, plane_mid)
    end = send(two, plane_end)
    return two, (pair, mid, end)


def local_lines(
    tokens,
    norm_gain,
    query_weight,
    key_weight,
    value_weight,
    pool_in_weight,
    pool_mix_weight,
    sink_logit,
    out_pool_weight,
    out_attn_weight,
):
    _, y, _, c = position()
    home = y == c
    tok_rows = tokens.shape[0]
    seq_total = tok_rows * lax.axis_size("sp")

    rest = pack((key_weight, value_weight, pool_in_weight), 1)
    in_sent = (send(query_weight, swap_away), send(rest, swap_away))
    in_shape = (query_weight.shape[0], query_weight.shape[1] + rest.shape[1])
    in_cur = choose((query_weight, rest), in_sent, 1, in_shape)
    in_two, in_far = line_gather(in_cur)

    px = send(tokens, flip_x)
    py = send(tokens, flip_y)
    pxy = send(py, flip_x)

    mix = pool_mix_weight[0]
    w_out = pack((out_pool_weight, out_attn_weight, mix), 0)
    out_swapped = send(w_out, swap_away)
    sink_other = send(sink_logit, swap_away)
    cut = w_out.shape[0] - mix.shape[0]
    out_cur = choose((w_out,), (out_swapped,), 0, (cut, w_out.shape[1]))
    out_two, out_far = line_gather(out_cur)

    pieces = (tokens, px, py, pxy)
    stats = row_stats(pieces)
    keep, give = prepare(pieces, stats, send(stats, other_core), norm_gain[None, :])
    got = send(give, other_core)
    own_acc, other_acc = project_near(keep, got, in_cur, in_two)
    q_w, kv_w, pool_w = query_weight.shape[1], key_weight.shape[1], pool_in_weight.shape[1]
    tables = turn_tables(tok_rows)
    a_part = send(project_other(q_w, 2 * kv_w + pool_w, keep, got, other_acc, in_far), other_core)
    b_part = send(project_other(0, q_w, keep, got, other_acc, in_far), other_core)
    edge = (WINDOW + pool_reach, pool_w)
    outs = ((tok_rows, 2 * kv_w), (tok_rows, pool_w), edge, edge)
    pair, pool_input, near, far = project_own(pair_kernel, q_w, keep, got, own_acc, tables, a_part, in_far, outs)
    (query,) = project_own(query_kernel, 0, keep, got, own_acc, tables, b_part, in_far, ((tok_rows, q_w),))
    inside = send(near, other_core)
    outside = send(far, across_planes)
    acts, log_here = attend(query, pair, pool_input, inside, outside, mix, out_swapped[cut:], sink_logit, sink_other, seq_total)
    log_weight = jnp.where(home, log_here, send(log_here, swap_away))

    acts_other = send(acts, other_core)
    sums = []
    for late in (False, True):
        blocks = out_blocks(late, acts, acts_other, out_far if late else (out_cur, out_two))
        parts = [blocks[0]]
        for r, rule in ((1, flip_x), (2, flip_y), (3, flip_xy)):
            parts.append(send(blocks[r], rule))
        sums.append(sum_parts(parts))
    early_other = send(sums[0], give_early)
    late_other = send(sums[1], give_late)
    mixed = assemble(sums[0], sums[1], early_other, late_other)
    return (mixed, log_weight)


def solution(mesh):
    lines = mesh.shape["sp"] == 8 and mesh.shape["tp"] == 4
    return jax.shard_map(
        local_lines if lines else local,
        mesh=mesh,
        in_specs=(
            P("sp", "tp"),
            P(),
            P("sp", "tp"),
            P("sp", "tp"),
            P("sp", "tp"),
            P("sp", "tp"),
            P("tp", None, None),
            P("tp"),
            P("tp", "sp"),
            P("tp", "sp"),
        ),
        out_specs=(P("sp", "tp"), P("tp", "sp")),
        check_vma=False,
    )
```
